32 devices in a mesh: sp: 8 (over z, x), tp: 4 (over y, core).
Axes of the slice: x: 2, y: 2, z: 4, core: 2. Of those that a mesh axis runs over, the one named last changes fastest.
Arguments:
- lane_source_signal: bfloat16 [1024, 1024], P('tp', 'sp'), may hold values from -6 to 6
- spectral_damping_part: float32 [64, 64], P('tp'), may hold values from -3 to -0.0002
- spectral_angular_part: float32 [64, 64], P('tp'), may hold values from 0.31 to 201.0624
- interval_exponent: float32 [64], P('tp'), may hold values from -3.9 to -1.6
- entry_matrix_inphase: float32 [64, 64, 16], P('tp'), may hold values from -1 to 1
- entry_matrix_quadrature: float32 [64, 64, 16], P('tp'), may hold values from -1 to 1
- emission_inphase: float32 [64, 16, 64], P('tp'), may hold values from -0.75 to 0.75
- emission_quadrature: float32 [64, 16, 64], P('tp'), may hold values from -0.75 to 0.75
- lane_bypass_factor: float32 [1024], P('tp'), may hold values from -5 to 5
- spike_shrink_offset: float32 [64, 1024], P('tp', 'sp'), may hold values from -1.4 to 0
- lane_exit_matrix: bfloat16 [1024, 4096], P('tp'), may hold values from -0.1875 to 0.1875
- skipline_stream: bfloat16 [1024, 4096], P('sp'), may hold values from -6 to 6
- specialist_scaling_vector: float32 [4096], replicated, may hold values from 0.1 to 1.9
- selected_specialists: int32 [1024, 2], P('sp'), may hold values from 0 to 7, all different within a row; in each aligned block of 128 rows (0 to 127, 128 to 255, ...) at most 64 rows name the same one
- dispatcher_scores: float32 [1024, 2], P('sp'), may hold values from 0.1 to 1
- specialist_valve_matrix: bfloat16 [8, 4096, 2048], P('sp', None, 'tp'), may hold values from -0.09375 to 0.09375
- specialist_widen_matrix: bfloat16 [8, 4096, 2048], P('sp', None, 'tp'), may hold values from -0.09375 to 0.09375
- specialist_shrink_matrix: bfloat16 [8, 2048, 4096], P('sp', 'tp'), may hold values from -0.1875 to 0.1875
Outputs:
- updated: bfloat16 [1024, 4096], P('sp', 'tp')
The draws below stay inside these ranges and needn't reach their ends.
Inputs may be any that keep to these rules, and one draw needn't show every extreme that they name: `selected_specialists`: each row names 2 different experts. Among the rows of each aligned block of 128 positions no expert is named more than 64 times, and in every block some expert is named exactly 64 times.
All inputs are finite; a program needn't handle non-finite values.
Results may differ from the reference program's by a relative error of at most 0.019.
Values may be sent and summed in bfloat16 or wider, within the bound.
No kernel may reach another device: no remote copies, remote signals or barrier semaphores. Data moves between devices by JAX's collectives and lax.ppermute only.
A program may use at most 64 MiB of HBM per device.

```python
import math
import jax
import jax.numpy as jnp
import numpy as np
from jax import lax

D = 4096
C = 1024
GS = 16
P_SIZE = 64
F = 2048
TOPK = 2
TOK_DEV = 128
G = 64
TOKENS = 1024
EXPERTS = 8
CAP = 64
N_SP = 8
N_TP = 4


def draw_spectral_damping_part(key, part):
    subkeys = jax.random.split(key, 3)
    fast_group = jax.random.uniform(subkeys[0], (G, 1)) < 0.5
    quick_rate = -jax.random.uniform(subkeys[1], (G, P_SIZE), jnp.float32, 1.0, 3.0)
    slow_rate = -jnp.exp(jax.random.uniform(subkeys[2], (G, P_SIZE), jnp.float32, math.log(0.0002), math.log(0.001)))
    return jnp.where(fast_group, quick_rate, slow_rate)


def draw_spectral_angular_part(key, part):
    offset = jax.random.uniform(key, (G, P_SIZE), jnp.float32, 0.1, 0.9)
    return math.pi * (jnp.arange(P_SIZE, dtype=jnp.float32)[None, :] + offset)


def draw_spike_shrink_offset(key, part):
    subkeys = jax.random.split(key, 3)
    blocks = TOKENS // 32
    block_rate = jnp.exp(jax.random.uniform(subkeys[0], (G, blocks), jnp.float32, math.log(2.5e-05), math.log(0.0001)))
    baseline = -jnp.repeat(block_rate, 32, axis=1)
    spots = jax.random.randint(subkeys[1], (G, 2), 0, TOKENS)
    losses = jnp.log(1.0 - jax.random.uniform(subkeys[2], (G, 2), jnp.float32, 0.2, 0.5))
    position = jnp.arange(TOKENS, dtype=jnp.int32)[None, :, None]
    struck = position == spots[:, None, :]
    return baseline + jnp.sum(jnp.where(struck, losses[:, None, :], 0.0), axis=2)


def raised(result, stream_key, source, target, shards_of, factor):
    owner, partner = [(jnp.arange(result.shape[dim]) // (result.shape[dim] // shards_of)).reshape([-1 if axis == dim else 1 for axis in range(result.ndim)]) for dim in (source, target)]
    chosen = jax.random.permutation(stream_key, shards_of)[partner]
    strong = (owner == chosen) | (owner == (partner + shards_of // 2) % shards_of)
    return jnp.where(strong, factor * result, result)


def steps_of(stream_key, shape, cuts, smallest, top_value):
    def one(dim, shards_of):
        steps = jax.random.uniform(jax.random.fold_in(jax.random.fold_in(stream_key, 6), dim), (shards_of,), jnp.float32, smallest / len(cuts), top_value / len(cuts))
        return jnp.repeat(jnp.exp(steps), shape[dim] // shards_of).reshape((-1,) + (1,) * (len(shape) - dim - 1))

    factor_of = one(*cuts[0])
    for cut in cuts[1:]:
        factor_of = factor_of * one(*cut)
    return factor_of


def assign_block(rng, own, number, rows, number_of, top, most, skew):
    sequence = jax.random.permutation(rng, number_of)
    crowded, common = shares(number_of, rows * top, most, skew, True), shares(number_of, rows * top, most, skew, False)
    places = jnp.arange(number_of)

    def named(tallies, turn):
        used = int((tallies > 0).sum())
        fixed = max(1, used // 4)
        moved = fixed + (places - fixed + turn * (used - fixed)) % max(1, number_of - fixed)
        return jnp.zeros((number_of,), jnp.int32).at[sequence[jnp.where(places < fixed, places, moved)]].set(jnp.asarray(tallies, jnp.int32))

    tallies = jnp.where(number % 4 == 0, named(crowded, number // 4), named(common, number - number // 4 - 1))
    mixed = jax.random.permutation(jax.random.fold_in(own, 3), number_of)
    giver, sink = mixed[0:number_of // 2 * 2:2], mixed[1:number_of // 2 * 2:2]
    slack = jnp.minimum(tallies[giver] - 1, most - tallies[sink]) // 2
    slack = jnp.where((giver == sequence[0]) | (sink == sequence[0]) | (tallies[sink] == 0), 0, jnp.maximum(slack, 0))
    moved = jax.random.randint(jax.random.fold_in(own, 4), (number_of // 2,), 0, 1 << 20) % (slack + 1)
    tallies = tallies.at[giver].add(-moved).at[sink].add(moved)
    members = jnp.searchsorted(jnp.cumsum(tallies), jnp.arange(rows * top), side="right").astype(jnp.int32)
    listing = members.reshape(top, rows).T
    listing = listing[jax.random.permutation(jax.random.fold_in(own, 1), rows)]
    turn = jax.random.randint(jax.random.fold_in(own, 2), (rows, 1), 0, top)
    return jnp.take_along_axis(listing, (jnp.arange(top)[None, :] + turn) % top, axis=1)


def shares(number_of, total, reach, lean, full):
    loads = [(1 << 20) // math.isqrt(grade ** lean) + 1 for grade in range(1, number_of + 1)]
    largest = reach if full else min(reach, max(-(-total // number_of), total * loads[0] // sum(loads)))
    least = 1 if total - largest >= number_of - 1 else 0
    given, surplus = [largest] + [least] * (number_of - 1), total - largest - least * (number_of - 1)
    while surplus > 0:
        free = [i for i in range(1, number_of) if given[i] < largest] or [i for i in range(1, number_of) if given[i] < reach]
        whole, left = sum([loads[i] for i in free]), surplus
        for i in free:
            more = min(reach - given[i], max(1, left * loads[i] // whole), surplus)
            given[i] = given[i] + more
            surplus = surplus - more
    return np.array(given)


def centred(key, shape, width, most, pieces=(), kind=jnp.bfloat16):
    gain = steps_of(key, shape, pieces, -0.22, 0.18) if pieces else 1.0
    result = jax.random.normal(key, shape, jnp.float32) * width * gain
    return jnp.minimum(jnp.maximum(result, -most), most).astype(kind)


def heavy_noise(own_key, extent, width, most, shards, heavy, kind=jnp.bfloat16):
    array = width * jax.random.normal(own_key, extent, jnp.float32)
    if shards:
        array = array * steps_of(own_key, extent, shards, -0.22, 0.18)
    return jnp.clip(raised(array, jax.random.fold_in(own_key, 3), *heavy), -most, most).astype(kind)


def setup_inputs(seed: int = 0) -> dict:
    streams_of = jax.random.split(jax.random.key(seed), 19)
    lane_source_signal = centred(streams_of[0], (C, TOKENS), 1.0, 6.0, ((0, 4), (1, 8)))
    spectral_damping_part = draw_spectral_damping_part(jax.random.fold_in(streams_of[18], 71), 0)
    spectral_angular_part = draw_spectral_angular_part(jax.random.fold_in(streams_of[18], 71), 0)
    interval_exponent = jnp.clip(-3.9 + 2.3000001 * jax.random.uniform(streams_of[3], (G,), jnp.float32) ** steps_of(streams_of[3], (G,), ((0, 4),), -0.2, 0.2), -3.9, -1.6)
    entry_matrix_inphase = centred(streams_of[4], (G, P_SIZE, GS), (2 * GS) ** -0.5, 1.0, ((0, 4),), jnp.float32)
    entry_matrix_quadrature = centred(streams_of[5], (G, P_SIZE, GS), (2 * GS) ** -0.5, 1.0, ((0, 4),), jnp.float32)
    emission_inphase = centred(streams_of[6], (G, GS, P_SIZE), P_SIZE ** -0.5, 0.75, ((0, 4),), jnp.float32)
    emission_quadrature = centred(streams_of[7], (G, GS, P_SIZE), P_SIZE ** -0.5, 0.75, ((0, 4),), jnp.float32)
    lane_bypass_factor = centred(streams_of[8], (C,), 1.0, 5.0, ((0, 4),), jnp.float32)
    spike_shrink_offset = draw_spike_shrink_offset(jax.random.fold_in(streams_of[18], 71), 0)
    lane_exit_matrix = centred(streams_of[10], (C, D), C ** -0.5, 0.1875, ((0, 4),))
    skipline_stream = centred(streams_of[11], (TOKENS, D), 1.0, 6.0, ((0, 8),))
    specialist_scaling_vector = jnp.clip(1.0 + 0.18 * jax.random.normal(streams_of[12], (D,), jnp.float32), 0.1, 1.9)
    selected_specialists_keys = jax.random.split(jax.random.fold_in(streams_of[13], 1), TOKENS // TOK_DEV)
    selected_specialists_turns = jax.random.permutation(jax.random.fold_in(streams_of[13], 3), TOKENS // TOK_DEV)
    selected_specialists = jax.vmap(lambda own, number: assign_block(jax.random.fold_in(streams_of[13], 2), own, number, TOK_DEV, EXPERTS, TOPK, CAP, 2))(selected_specialists_keys, selected_specialists_turns).reshape((TOKENS, TOPK))
    dispatcher_scores = jnp.clip(jnp.exp(math.log(1.0) - 2.3025851 * jax.random.uniform(streams_of[14], (TOKENS, TOPK), jnp.float32) ** steps_of(streams_of[14], (TOKENS, TOPK), ((0, 8),), -0.2, 0.2)), 0.1, 1.0)
    specialist_valve_matrix = centred(streams_of[15], (EXPERTS, D, F), D ** -0.5, 0.09375, ((0, 8), (2, 4)))
    specialist_widen_matrix = centred(streams_of[16], (EXPERTS, D, F), D ** -0.5, 0.09375, ((0, 8), (2, 4)))
    specialist_shrink_matrix = heavy_noise(streams_of[17], (EXPERTS, F, D), F ** -0.5, 0.1875, ((0, 8), (1, 4)), (1, 2, 4, 2.0))
    return {"lane_source_signal": lane_source_signal, "spectral_damping_part": spectral_damping_part, "spectral_angular_part": spectral_angular_part, "interval_exponent": interval_exponent, "entry_matrix_inphase": entry_matrix_inphase, "entry_matrix_quadrature": entry_matrix_quadrature, "emission_inphase": emission_inphase, "emission_quadrature": emission_quadrature, "lane_bypass_factor": lane_bypass_factor, "spike_shrink_offset": spike_shrink_offset, "lane_exit_matrix": lane_exit_matrix, "skipline_stream": skipline_stream, "specialist_scaling_vector": specialist_scaling_vector, "selected_specialists": selected_specialists, "dispatcher_scores": dispatcher_scores, "specialist_valve_matrix": specialist_valve_matrix, "specialist_widen_matrix": specialist_widen_matrix, "specialist_shrink_matrix": specialist_shrink_matrix}


EPS = 1e-06
PRECISE_MODE = lax.Precision.HIGHEST

def affine_pair(earlier, latter):
    mul_re = earlier[0] * latter[0] - earlier[1] * latter[1]
    mul_im = earlier[0] * latter[1] + earlier[1] * latter[0]
    add_re = latter[0] * earlier[2] - latter[1] * earlier[3] + latter[2]
    add_im = latter[0] * earlier[3] + latter[1] * earlier[2] + latter[3]
    return (mul_re, mul_im, add_re, add_im)

def bundled_recurrence_layer(packed):
    u_group, a_real, a_imag, log_dt, b_real, b_imag, c_real, c_imag, skip_group, extra_row = packed
    step_size = jnp.exp(log_dt)
    natural_pace_exponent = a_real * step_size
    angle = a_imag * step_size
    num_re = jnp.expm1(natural_pace_exponent) * jnp.cos(angle) - 2.0 * jnp.sin(0.5 * angle) ** 2
    num_im = jnp.exp(natural_pace_exponent) * jnp.sin(angle)
    denom = a_real * a_real + a_imag * a_imag
    fac_re = (num_re * a_real + num_im * a_imag) / denom
    fac_im = (num_im * a_real - num_re * a_imag) / denom
    map_re = fac_re[:, None] * b_real - fac_im[:, None] * b_imag
    map_im = fac_re[:, None] * b_imag + fac_im[:, None] * b_real
    drive_re = jnp.dot(map_re, u_group, precision=PRECISE_MODE)
    drive_im = jnp.dot(map_im, u_group, precision=PRECISE_MODE)
    recurrence_modulus = jnp.exp(natural_pace_exponent[:, None] + extra_row[None, :])
    trans_re = recurrence_modulus * jnp.cos(angle)[:, None]
    trans_im = recurrence_modulus * jnp.sin(angle)[:, None]
    scanned = lax.associative_scan(affine_pair, (trans_re, trans_im, drive_re, drive_im), axis=1)
    value = jnp.dot(c_real, scanned[2], precision=PRECISE_MODE) - jnp.dot(c_imag, scanned[3], precision=PRECISE_MODE) + skip_group[:, None] * u_group
    return jax.nn.gelu(value).astype(jnp.bfloat16)

def reference(lane_source_signal, spectral_damping_part, spectral_angular_part, interval_exponent, entry_matrix_inphase, entry_matrix_quadrature, emission_inphase, emission_quadrature, lane_bypass_factor, spike_shrink_offset, lane_exit_matrix, skipline_stream, specialist_scaling_vector, selected_specialists, dispatcher_scores, specialist_valve_matrix, specialist_widen_matrix, specialist_shrink_matrix):
    f32 = jnp.float32
    bf16 = jnp.bfloat16
    bundle_total = spectral_damping_part.shape[0]
    lanes_within_bundle = entry_matrix_inphase.shape[2]
    length = lane_source_signal.shape[1]
    bundled_signal = lane_source_signal.astype(f32).reshape(bundle_total, lanes_within_bundle, length)
    recurrence_result = lax.map(bundled_recurrence_layer, (bundled_signal, spectral_damping_part, spectral_angular_part, interval_exponent, entry_matrix_inphase, entry_matrix_quadrature, emission_inphase, emission_quadrature, lane_bypass_factor.reshape(bundle_total, lanes_within_bundle), spike_shrink_offset))
    recurrence_result = recurrence_result.reshape(bundle_total * lanes_within_bundle, length)
    projected = jnp.dot(recurrence_result.T, lane_exit_matrix, preferred_element_type=f32).astype(bf16)
    stream = (skipline_stream.astype(f32) + lax.optimization_barrier(projected).astype(f32)).astype(bf16)
    stream_f = lax.optimization_barrier(stream).astype(f32)
    inv_rms = lax.rsqrt(lax.optimization_barrier(jnp.mean(stream_f * stream_f, axis=-1, keepdims=True)) + EPS)
    normed = (stream_f * inv_rms * specialist_scaling_vector).astype(bf16)
    share = dispatcher_scores / lax.optimization_barrier(jnp.sum(dispatcher_scores, axis=1, keepdims=True))
    flat_routes = selected_specialists.reshape(-1)
    flat_share = share.reshape(-1)
    slots = N_SP * CAP
    block_units = F // N_TP

    def one_expert(total, packed):
        gate_w, up_w, down_w, expert_id = packed
        chosen = flat_routes == expert_id
        positions = jnp.nonzero(chosen, size=slots, fill_value=0)[0].astype(jnp.int32)
        valid = jnp.arange(slots, dtype=jnp.int32) < jnp.sum(chosen.astype(jnp.int32))
        token_ids = positions // TOPK
        rows = normed[token_ids]
        gate_part = jnp.dot(rows, gate_w, preferred_element_type=f32)
        up_part = jnp.dot(rows, up_w, preferred_element_type=f32)
        hidden = (jax.nn.silu(gate_part) * up_part).astype(bf16)
        hidden_blocks = jnp.transpose(hidden.reshape(slots, N_TP, block_units), (1, 0, 2))
        down_blocks = down_w.reshape(N_TP, block_units, down_w.shape[1])

        def add_block(acc, pair):
            part = jnp.dot(pair[0], pair[1], preferred_element_type=f32).astype(bf16)
            return (acc + lax.optimization_barrier(part).astype(f32), None)
        acc0 = jnp.zeros((slots, down_w.shape[1]), f32)
        summed, _ = lax.scan(add_block, acc0, (hidden_blocks, down_blocks))
        expert_out = lax.optimization_barrier(summed.astype(bf16)).astype(f32)
        weights = jnp.where(valid, flat_share[positions], 0.0)
        return (total.at[token_ids].add(weights[:, None] * expert_out), None)
    start = jnp.zeros(stream_f.shape, f32)
    experts = specialist_valve_matrix.shape[0]
    moe, _ = lax.scan(one_expert, start, (specialist_valve_matrix, specialist_widen_matrix, specialist_shrink_matrix, jnp.arange(experts, dtype=jnp.int32)))
    return (stream_f + moe).astype(bf16)
```

```python
import jax
import jax.numpy as jnp
from jax import lax
from jax.experimental import pallas as pl
from jax.experimental.pallas import tpu as pltpu
from jax.sharding import PartitionSpec as P

EPS = 1e-06
PRECISE_MODE = lax.Precision.HIGHEST
HALVES = 2
F32 = jnp.float32
BF16 = jnp.bfloat16


def swap(value, axis, bits):
    count = lax.axis_size(axis)
    return lax.ppermute(value, axis, [(i, i ^ bits) for i in range(count)])


def affine_pair(earlier, latter):
    mul_re = earlier[0] * latter[0] - earlier[1] * latter[1]
    mul_im = earlier[0] * latter[1] + earlier[1] * latter[0]
    add_re = latter[0] * earlier[2] - latter[1] * earlier[3] + latter[2]
    add_im = latter[0] * earlier[3] + latter[1] * earlier[2] + latter[3]
    return (mul_re, mul_im, add_re, add_im)


def local_prefix(elements):
    length = elements[0].shape[2]
    fills = (1.0, 0.0, 0.0, 0.0)
    offset = 1
    while offset < length:
        earlier = tuple(
            (
                jnp.pad(
                    item[:, :, : length - offset],
                    ((0, 0), (0, 0), (offset, 0)),
                    constant_values=fill,
                )
                for item, fill in zip(elements, fills)
            )
        )
        elements = affine_pair(earlier, elements)
        offset = offset * 2
    return elements


def carried_in(summary):
    count, mine = lax.axis_size("sp"), lax.axis_index("sp")
    pieces = lax.all_to_all(
        jnp.broadcast_to(summary[None], (count,) + summary.shape), "sp", 0, 0, tiled=True
    )

    def lap(position, running):
        mul_re, mul_im, add_re, add_im = (pieces[position, i] for i in range(4))
        re, im = running
        longer = (mul_re * re - mul_im * im + add_re, mul_re * im + mul_im * re + add_im)
        return jax.tree.map(lambda new, old: jnp.where(position < mine, new, old), longer, running)

    blank = jnp.zeros_like(summary[0])
    return lax.fori_loop(0, count - 1, lap, (blank, blank))


def ffn_kernel(n_tp, width, t_ref, *refs):
    pieces = refs[:n_tp]
    scale_ref, gate_ref, up_ref, down_ref, out_ref, gate_acc, up_acc, square_acc, hidden_ref = refs[n_tp:]
    step = pl.program_id(0)
    for k in range(n_tp):

        @pl.when(step == k)
        def _():
            rows = pieces[k][...].astype(F32)
            square = jnp.sum(rows * rows, axis=1, keepdims=True)
            scaled = (rows * scale_ref[0]).astype(BF16)
            gate = jnp.dot(scaled, gate_ref[...], preferred_element_type=F32)
            up = jnp.dot(scaled, up_ref[...], preferred_element_type=F32)
            if k > 0:
                square = square + square_acc[...]
                gate = gate + gate_acc[...]
                up = up + up_acc[...]
            if k < n_tp - 1:
                square_acc[...] = square
                gate_acc[...] = gate
                up_acc[...] = up
            else:
                inv_rms = lax.rsqrt(square / width + EPS)
                gate = gate * inv_rms
                up = up * inv_rms
                hidden_ref[...] = (gate * jax.nn.sigmoid(gate) * up).astype(BF16)

    @pl.when(step >= n_tp)
    def _():
        out_ref[0] = jnp.dot(
            hidden_ref[...], down_ref[...], preferred_element_type=F32
        ).astype(BF16)


def ffn(pieces, scale, gate_w, up_w, down_w, me):
    n_tp = len(pieces)
    rows, d_local = pieces[0].shape
    width, units = gate_w.shape

    def early(i, t):
        return jnp.bitwise_xor(t[0], jnp.minimum(i, n_tp - 1))

    def late(i, t):
        return jnp.bitwise_xor(t[0], jnp.maximum(i - n_tp, 0))

    whole = pl.BlockSpec((rows, d_local), lambda i, t: (0, 0))
    return pl.pallas_call(
        lambda *refs: ffn_kernel(n_tp, width, *refs),
        grid_spec=pltpu.PrefetchScalarGridSpec(
            num_scalar_prefetch=1,
            grid=(2 * n_tp,),
            in_specs=[whole] * n_tp
            + [
                pl.BlockSpec((1, 1, d_local), lambda i, t: (early(i, t), 0, 0)),
                pl.BlockSpec((d_local, units), lambda i, t: (early(i, t), 0)),
                pl.BlockSpec((d_local, units), lambda i, t: (early(i, t), 0)),
                pl.BlockSpec((units, d_local), lambda i, t: (0, late(i, t))),
            ],
            out_specs=pl.BlockSpec(
                (1, rows, d_local), lambda i, t: (jnp.maximum(i - n_tp, 0), 0, 0)
            ),
            scratch_shapes=[
                pltpu.VMEM((rows, units), F32),
                pltpu.VMEM((rows, units), F32),
                pltpu.VMEM((rows, 1), F32),
                pltpu.VMEM((rows, units), BF16),
            ],
        ),
        out_shape=jax.ShapeDtypeStruct((n_tp, rows, d_local), BF16),
        compiler_params=pltpu.CompilerParams(dimension_semantics=("arbitrary",)),
        cost_estimate=pl.CostEstimate(
            flops=6 * rows * width * units,
            bytes_accessed=6 * width * units + 4 * rows * width,
            transcendentals=rows * units,
        ),
        name="expert_ffn",
    )(me.reshape(1), *pieces, scale, gate_w, up_w, down_w)


def gather_pieces(own, n_tp):
    pieces = {0: own}
    bit = n_tp // 2
    while bit:
        for k in list(pieces):
            pieces[k ^ bit] = swap(pieces[k], "tp", bit)
        bit //= 2
    return [pieces[k] for k in range(n_tp)]


def scatter_sum(parts, n_tp):
    held = {k: parts[k] for k in range(n_tp)}
    bit = 1
    while bit < n_tp:
        for k in sorted(held):
            if k & bit:
                moved = swap(held[k], "tp", bit).astype(F32)
                held[k ^ bit] = (held[k ^ bit].astype(F32) + moved).astype(BF16)
        held = {k: v for k, v in held.items() if not k & bit}
        bit *= 2
    return held[0]


def per_device(
    lane_source_signal,
    spectral_damping_part,
    spectral_angular_part,
    interval_exponent,
    entry_matrix_inphase,
    entry_matrix_quadrature,
    emission_inphase,
    emission_quadrature,
    lane_bypass_factor,
    spike_shrink_offset,
    lane_exit_matrix,
    skipline_stream,
    specialist_scaling_vector,
    selected_specialists,
    dispatcher_scores,
    specialist_valve_matrix,
    specialist_widen_matrix,
    specialist_shrink_matrix,
):
    n_tp, me = lax.axis_size("tp"), lax.axis_index("tp")
    width = specialist_scaling_vector.shape[0]
    d_local = width // n_tp
    groups_here = spectral_damping_part.shape[0]
    lanes_within_bundle = entry_matrix_inphase.shape[2]
    tok_local = lane_source_signal.shape[1]

    exits = []
    for k in range(n_tp):
        block = lax.dynamic_slice_in_dim(lane_exit_matrix, (me ^ k) * d_local, d_local, 1)
        exits.append(swap(block, "tp", k) if k else block)

    bundled_signal = lane_source_signal.astype(F32).reshape(
        groups_here, lanes_within_bundle, tok_local
    )
    step_size = jnp.exp(interval_exponent)[:, None]
    natural_pace_exponent = spectral_damping_part * step_size
    angle = spectral_angular_part * step_size
    num_re = jnp.expm1(natural_pace_exponent) * jnp.cos(angle) - 2.0 * jnp.sin(0.5 * angle) ** 2
    num_im = jnp.exp(natural_pace_exponent) * jnp.sin(angle)
    denom = (
        spectral_damping_part * spectral_damping_part
        + spectral_angular_part * spectral_angular_part
    )
    fac_re = (num_re * spectral_damping_part + num_im * spectral_angular_part) / denom
    fac_im = (num_im * spectral_damping_part - num_re * spectral_angular_part) / denom
    map_re = (
        fac_re[:, :, None] * entry_matrix_inphase - fac_im[:, :, None] * entry_matrix_quadrature
    )
    map_im = (
        fac_re[:, :, None] * entry_matrix_quadrature + fac_im[:, :, None] * entry_matrix_inphase
    )
    drive_re = jnp.einsum("gpc,gct->gpt", map_re, bundled_signal, precision=PRECISE_MODE)
    drive_im = jnp.einsum("gpc,gct->gpt", map_im, bundled_signal, precision=PRECISE_MODE)
    recurrence_modulus = jnp.exp(
        natural_pace_exponent[:, :, None] + spike_shrink_offset[:, None, :]
    )
    trans_re = recurrence_modulus * jnp.cos(angle)[:, :, None]
    trans_im = recurrence_modulus * jnp.sin(angle)[:, :, None]
    cum_re, cum_im, state_real, state_imaginary = local_prefix(
        (trans_re, trans_im, drive_re, drive_im)
    )
    summary = jnp.stack(
        [part[:, :, -1] for part in (cum_re, cum_im, state_real, state_imaginary)]
    )
    enter_re, enter_im = carried_in(summary)
    enter_re = enter_re[:, :, None]
    enter_im = enter_im[:, :, None]
    state_real = state_real + cum_re * enter_re - cum_im * enter_im
    state_imaginary = state_imaginary + cum_re * enter_im + cum_im * enter_re
    value = (
        jnp.einsum("nef,nfi->nei", emission_inphase, state_real, precision=PRECISE_MODE)
        - jnp.einsum("nef,nfi->nei", emission_quadrature, state_imaginary, precision=PRECISE_MODE)
        + lane_bypass_factor.reshape(groups_here, lanes_within_bundle)[:, :, None] * bundled_signal
    )
    mixed = jax.nn.gelu(value).astype(BF16).reshape(groups_here * lanes_within_bundle, tok_local)

    projected = 0.0
    for k in range(n_tp):
        other = swap(mixed, "tp", k) if k else mixed
        projected = projected + jnp.einsum(
            "ct,cd->td", other, exits[k], preferred_element_type=F32
        )
    own_skip = lax.dynamic_slice_in_dim(skipline_stream, me * d_local, d_local, 1)
    stream = (own_skip.astype(F32) + projected.astype(BF16).astype(F32)).astype(BF16)

    share = dispatcher_scores / jnp.sum(dispatcher_scores, axis=1, keepdims=True)
    experts = lax.axis_size("sp")
    top = selected_specialists.shape[1]
    capacity = 2 * tok_local * top // experts
    part_slots = capacity // HALVES
    chosen = [
        selected_specialists[:, k : k + 1] == jnp.arange(experts, dtype=jnp.int32)[None, :]
        for k in range(top)
    ]
    counted = sum(c.astype(jnp.int32) for c in chosen)
    ranks = jnp.cumsum(counted, axis=0) - counted
    slots = [jnp.sum(jnp.where(c, ranks, 0), axis=1) for c in chosen]

    gate_w = specialist_valve_matrix[0]
    up_w = specialist_widen_matrix[0]
    down_w = specialist_shrink_matrix[0]
    scale = specialist_scaling_vector.reshape(n_tp, 1, d_local)

    grid = jnp.arange(experts * part_slots, dtype=jnp.int32)
    arrived = []
    places = []
    for h in range(HALVES):
        keys = [
            jnp.where(
                (slots[k] >= h * part_slots) & (slots[k] < (h + 1) * part_slots),
                selected_specialists[:, k] * part_slots + slots[k] - h * part_slots,
                -1,
            )
            for k in range(top)
        ]
        places.append(keys)
        pick = sum((grid[:, None] == key[None, :]).astype(BF16) for key in keys)
        rows = jnp.dot(pick, stream, preferred_element_type=F32).astype(BF16)
        arrived.append(
            lax.all_to_all(
                rows.reshape(experts, part_slots, d_local), "sp", 0, 0, tiled=True
            ).reshape(experts * part_slots, d_local)
        )
    combined = stream.astype(F32)
    for h in range(HALVES):
        pieces = gather_pieces(arrived[h], n_tp)
        parts = ffn(pieces, scale, gate_w, up_w, down_w, me)
        expert_out = scatter_sum(parts, n_tp)
        returned = lax.all_to_all(
            expert_out.reshape(experts, part_slots, d_local), "sp", 0, 0, tiled=True
        ).reshape(experts * part_slots, d_local)
        weight = sum(
            jnp.where(key[:, None] == grid[None, :], share[:, k : k + 1], 0.0)
            for k, key in enumerate(places[h])
        )
        high = weight.astype(BF16)
        low = (weight - high.astype(F32)).astype(BF16)
        combined = (
            combined
            + jnp.dot(high, returned, preferred_element_type=F32)
            + jnp.dot(low, returned, preferred_element_type=F32)
        )
    return combined.astype(BF16)


def solution(mesh):
    placed = (
        P("tp", "sp"),
        P("tp", None),
        P("tp", None),
        P("tp"),
        P("tp", None, None),
        P("tp", None, None),
        P("tp", None, None),
        P("tp", None, None),
        P("tp"),
        P("tp", "sp"),
        P("tp", None),
        P("sp", None),
        P(),
        P("sp", None),
        P("sp", None),
        P("sp", None, "tp"),
        P("sp", None, "tp"),
        P("sp", "tp", None),
    )
    return jax.shard_map(
        per_device, mesh=mesh, in_specs=placed, out_specs=P("sp", "tp"), check_vma=False
    )
```

```python
import jax
import jax.numpy as jnp
from jax import lax
from jax.experimental import pallas as pl
from jax.experimental.pallas import tpu as pltpu
from jax.sharding import PartitionSpec as P

EPS = 1e-06
F32 = jnp.float32
BF16 = jnp.bfloat16


def swap(value, axis, bits):
    count = lax.axis_size(axis)
    return lax.ppermute(value, axis, [(i, i ^ bits) for i in range(count)])


def expanded(columns, wide):
    return jnp.concatenate(
        [
            jnp.broadcast_to(columns[:, g : g + 1], (columns.shape[0], wide))
            for g in range(columns.shape[1])
        ],
        axis=1,
    )


def later(value, offset):
    if offset % 8:
        return pltpu.roll(value, offset, axis=0)
    return jnp.concatenate([value[-offset:], value[:-offset]], axis=0)


def block_rows(matrix, copies, inner):
    _, wide = matrix.shape
    spread = (
        lax.broadcasted_iota(jnp.int32, (wide, copies * wide), 1) % wide
        == lax.broadcasted_iota(jnp.int32, (wide, copies * wide), 0)
    ).astype(BF16)
    tiled = jnp.dot(matrix.astype(BF16), spread, preferred_element_type=F32)
    keep = (
        lax.broadcasted_iota(jnp.int32, tiled.shape, 0) // inner
        == lax.broadcasted_iota(jnp.int32, tiled.shape, 1) // wide
    )
    return jnp.where(keep, tiled, 0.0).astype(BF16)


def across(left, right):
    return lax.dot_general(left, right, (((1,), (1,)), ((), ())), preferred_element_type=F32)


def scan_kernel(
    signal_ref, damp_ref, turn_ref, pace_ref, ent_re_ref, ent_im_ref, shrink_ref,
    emit_re_ref, emit_im_ref, bypass_ref,
    summary_ref, local_ref, powers_ref, gone_ref,
):
    groups, states = damp_ref.shape
    length = shrink_ref.shape[1]
    lanes = ent_re_ref.shape[1]
    total = groups * states
    square = (groups, groups)
    step = jnp.where(
        lax.broadcasted_iota(jnp.int32, square, 0) == lax.broadcasted_iota(jnp.int32, square, 1),
        jnp.broadcast_to(pace_ref[...], square),
        0.0,
    )
    step = jnp.exp(jnp.sum(step, axis=1, keepdims=True))
    damp, turn = damp_ref[...], turn_ref[...]
    rate, angle = damp * step, turn * step
    size, cosine, sine = jnp.exp(rate), jnp.cos(angle), jnp.sin(angle)
    half = jnp.sin(0.5 * angle)
    series = rate * (1.0 + rate * 0.5 * (1.0 + rate * (1.0 / 3.0) * (1.0 + rate * 0.25)))
    less_one = jnp.where(jnp.abs(rate) < 0.05, series, size - 1.0)
    num_re = less_one * cosine - 2.0 * half * half
    num_im = size * sine
    denom = damp * damp + turn * turn
    own_group = (
        lax.broadcasted_iota(jnp.int32, (groups, total), 1) // states
        == lax.broadcasted_iota(jnp.int32, (groups, total), 0)
    )

    def row(value):
        spread = jnp.concatenate([value] * groups, axis=1)
        return jnp.sum(jnp.where(own_group, spread, 0.0), axis=0, keepdims=True)

    fac_re = row((num_re * damp + num_im * turn) / denom)
    fac_im = row((num_im * damp - num_re * turn) / denom)
    pow_re, pow_im = [row(size * cosine)], [row(num_im)]
    while 2 ** len(pow_re) < length:
        re, im = pow_re[-1], pow_im[-1]
        pow_re.append(re * re - im * im)
        pow_im.append(2.0 * re * im)
    for i, value in enumerate(pow_re + pow_im):
        powers_ref[i : i + 1, :] = value
    last = pow_re[-1], pow_im[-1]
    full_re = last[0] * last[0] - last[1] * last[1]
    full_im = 2.0 * last[0] * last[1]

    shrink = shrink_ref[...]
    summed = shrink
    position = lax.broadcasted_iota(jnp.int32, shrink.shape, 1)
    offset = 1
    while offset < length:
        summed = summed + jnp.where(
            position >= offset, pltpu.roll(summed, offset, axis=1), 0.0
        )
        offset *= 2
    columns = jnp.transpose(jnp.exp(jnp.concatenate([shrink, summed], axis=0)))
    gone_ref[...] = columns[:, groups:]
    all_gone = expanded(columns[length - 8 :, groups:], states)[7:8]
    flipped = jnp.transpose(signal_ref[...].astype(F32))
    local = bypass_ref[...] * flipped
    flipped = flipped.astype(BF16)
    ent_re = block_rows(ent_re_ref[...].reshape(groups * lanes, states), groups, lanes)
    ent_im = block_rows(ent_im_ref[...].reshape(groups * lanes, states), groups, lanes)
    emit_re = block_rows(emit_re_ref[...].reshape(groups * lanes, states), groups, lanes)
    emit_im = block_rows(emit_im_ref[...].reshape(groups * lanes, states), groups, lanes)
    wide = min(128, total)
    time = lax.broadcasted_iota(jnp.int32, (length, wide), 0)
    each = wide // states
    xs_re, xs_im = [], []
    for block in range(total // wide):
        cut = slice(block * wide, (block + 1) * wide)
        raw_re = jnp.dot(flipped, ent_re[:, cut], preferred_element_type=F32)
        raw_im = jnp.dot(flipped, ent_im[:, cut], preferred_element_type=F32)
        f_re, f_im = fac_re[:, cut], fac_im[:, cut]
        x_re = f_re * raw_re - f_im * raw_im
        x_im = f_re * raw_im + f_im * raw_re
        first = block * each
        decay = expanded(columns[:, first : first + each], states)
        decay = jnp.where(time >= 1, decay, 0.0)
        offset = 1
        for p_re, p_im in zip(pow_re, pow_im):
            a_re, a_im = p_re[:, cut], p_im[:, cut]
            s_re, s_im = later(x_re, offset), later(x_im, offset)
            x_re = x_re + decay * (a_re * s_re - a_im * s_im)
            x_im = x_im + decay * (a_re * s_im + a_im * s_re)
            if 2 * offset < length:
                decay = decay * later(decay, offset)
            offset *= 2
        local = local + across(x_re.astype(BF16), emit_re[:, cut])
        local = local - across(x_im.astype(BF16), emit_im[:, cut])
        xs_re.append(x_re[length - 8 :])
        xs_im.append(x_im[length - 8 :])
    local_ref[...] = local
    ends = []
    for value in (
        full_re * all_gone,
        full_im * all_gone,
        jnp.concatenate(xs_re, axis=1)[7:8],
        jnp.concatenate(xs_im, axis=1)[7:8],
    ):
        ends += [value[:, : total // 2], value[:, total // 2 :]]
    ends = jnp.concatenate(ends, axis=0)
    for s in range(summary_ref.shape[0]):
        summary_ref[s] = ends


def readout_kernel(
    mine_ref, pieces_ref, local_ref, powers_ref, gone_ref, emit_re_ref, emit_im_ref, mixed_ref
):
    groups, lanes, states = emit_re_ref.shape
    length, total = local_ref.shape[0], powers_ref.shape[1]
    mine = mine_ref[0]
    re = jnp.zeros((2, pieces_ref.shape[2]), F32)
    im = re
    for s in range(pieces_ref.shape[0] - 1):
        piece = pieces_ref[s]
        m_re, m_im, a_re, a_im = piece[0:2], piece[2:4], piece[4:6], piece[6:8]
        new_re = m_re * re - m_im * im + a_re
        new_im = m_re * im + m_im * re + a_im
        re = jnp.where(s < mine, new_re, re)
        im = jnp.where(s < mine, new_im, im)
    re = jnp.concatenate([re[0:1], re[1:2]], axis=1)
    im = jnp.concatenate([im[0:1], im[1:2]], axis=1)
    emit_re = block_rows(emit_re_ref[...].reshape(groups * lanes, states), groups, lanes)
    emit_im = block_rows(emit_im_ref[...].reshape(groups * lanes, states), groups, lanes)
    value = local_ref[...]
    bits = powers_ref.shape[0] // 2
    wide = min(128, total)
    each = wide // states
    near = lax.broadcasted_iota(jnp.int32, (8, wide), 0) + 1
    for block in range(total // wide):
        cut = slice(block * wide, (block + 1) * wide)
        p_re = [powers_ref[i : i + 1, cut] for i in range(bits)]
        p_im = [powers_ref[bits + i : bits + i + 1, cut] for i in range(bits)]
        c_re = jnp.broadcast_to(re[:, cut], (8, wide))
        c_im = jnp.broadcast_to(im[:, cut], (8, wide))
        for bit in range(4):
            a_re, a_im = p_re[bit], p_im[bit]
            on = (near >> bit) & 1 == 1
            c_re, c_im = (
                jnp.where(on, c_re * a_re - c_im * a_im, c_re),
                jnp.where(on, c_re * a_im + c_im * a_re, c_im),
            )
        bit = 3
        while c_re.shape[0] < length:
            a_re, a_im = p_re[bit], p_im[bit]
            c_re, c_im = (
                jnp.concatenate([c_re, c_re * a_re - c_im * a_im], axis=0),
                jnp.concatenate([c_im, c_re * a_im + c_im * a_re], axis=0),
            )
            bit += 1
        gone = expanded(gone_ref[:, block * each : (block + 1) * each], states)
        value = value + across((c_re * gone).astype(BF16), emit_re[:, cut])
        value = value - across((c_im * gone).astype(BF16), emit_im[:, cut])
    mixed_ref[...] = jax.nn.gelu(value).astype(BF16)


def vmem(count):
    return [pl.BlockSpec(memory_space=pltpu.VMEM)] * count


def hbm(count):
    return [pl.BlockSpec(memory_space=pltpu.HBM)] * count


def staged(kernel, first, count):
    def run(*refs):
        sources, buffers, sems = refs[first : first + count], refs[-count - 1 : -1], refs[-1]
        copies = [
            pltpu.make_async_copy(source, buffer, sems.at[i])
            for i, (source, buffer) in enumerate(zip(sources, buffers))
        ]
        for copy in copies:
            copy.start()
        for copy in copies:
            copy.wait()
        kernel(*refs[:first], *buffers, *refs[first + count : -count - 1])

    return run


def stage(args):
    return [pltpu.VMEM(arg.shape, arg.dtype) for arg in args] + [
        pltpu.SemaphoreType.DMA((len(args),))
    ]


def mixer(place, signal, damp, turn, pace, ent_re, ent_im, emit_re, emit_im, bypass, shrink):
    groups, states = damp.shape
    channels, length = signal.shape
    total = groups * states
    count = lax.axis_size("sp")
    bits = (length - 1).bit_length()
    args = (
        signal, damp, turn, pace.reshape(1, groups), ent_re.transpose(0, 2, 1),
        ent_im.transpose(0, 2, 1), shrink, emit_re, emit_im, bypass.reshape(1, channels),
    )
    summary, local, powers, gone = pl.pallas_call(
        staged(scan_kernel, 0, len(args)),
        in_specs=hbm(len(args)),
        out_specs=vmem(4),
        out_shape=[
            jax.ShapeDtypeStruct((count, 8, total // 2), F32),
            jax.ShapeDtypeStruct((length, channels), F32),
            jax.ShapeDtypeStruct((2 * bits, total), F32),
            jax.ShapeDtypeStruct((length, groups), F32),
        ],
        scratch_shapes=stage(args),
        compiler_params=pltpu.CompilerParams(vmem_limit_bytes=16 * 2**20),
        name="mixer_scan",
    )(*args)
    pieces = lax.all_to_all(summary, "sp", 0, 0, tiled=True)
    args = (emit_re, emit_im)
    return pl.pallas_call(
        staged(readout_kernel, 5, len(args)),
        in_specs=[pl.BlockSpec(memory_space=pltpu.SMEM)] + vmem(4) + hbm(len(args)),
        out_specs=vmem(1)[0],
        out_shape=jax.ShapeDtypeStruct((length, channels), BF16),
        scratch_shapes=stage(args),
        compiler_params=pltpu.CompilerParams(vmem_limit_bytes=16 * 2**20),
        name="mixer_readout",
    )(place, pieces, local, powers, gone, *args)


def cut_kernel(n_tp, place_ref, exit_ref, skip_ref, *refs):
    outs, sems = refs[: n_tp + 1], refs[n_tp + 1]
    me = place_ref[1]
    wide = outs[0].shape[1]
    copies = []
    for k in range(n_tp):
        source = exit_ref.at[:, pl.ds(pl.multiple_of((me ^ k) * wide, wide), wide)]
        copies.append(pltpu.make_async_copy(source, outs[k], sems.at[k]))
    source = skip_ref.at[:, pl.ds(pl.multiple_of(me * wide, wide), wide)]
    copies.append(pltpu.make_async_copy(source, outs[n_tp], sems.at[n_tp]))
    for copy in copies:
        copy.start()
    for copy in copies:
        copy.wait()


def cut_blocks(place, exit_matrix, skip, n_tp):
    wide = skip.shape[1] // n_tp
    block = jax.ShapeDtypeStruct((exit_matrix.shape[0], wide), BF16)
    anywhere = pl.BlockSpec(memory_space=pl.ANY)
    *exits, own_skip = pl.pallas_call(
        lambda *refs: cut_kernel(n_tp, *refs),
        in_specs=[pl.BlockSpec(memory_space=pltpu.SMEM)] + hbm(2),
        out_specs=[anywhere] * (n_tp + 1),
        out_shape=[block] * n_tp + [jax.ShapeDtypeStruct((skip.shape[0], wide), BF16)],
        scratch_shapes=[pltpu.SemaphoreType.DMA((n_tp + 1,))],
        compiler_params=pltpu.CompilerParams(vmem_limit_bytes=2**20),
        name="cut_blocks",
    )(place, exit_matrix, skip)
    return exits, own_skip


def route_kernel(experts, capacity, place_ref, chosen_ref, score_ref, pick_ref, high_ref, low_ref):
    chosen, score = chosen_ref[...], score_ref[...]
    length, top = chosen.shape
    share = score / jnp.sum(score, axis=1, keepdims=True)
    lane = lax.broadcasted_iota(jnp.int32, (length, experts), 1)
    named = [chosen[:, k : k + 1] == lane for k in range(top)]
    counted = sum(jnp.where(one, 1.0, 0.0) for one in named)
    before = (
        lax.broadcasted_iota(jnp.int32, (length, length), 0)
        > lax.broadcasted_iota(jnp.int32, (length, length), 1)
    )
    ranks = jnp.dot(
        jnp.where(before, 1.0, 0.0).astype(BF16), counted.astype(BF16),
        preferred_element_type=F32,
    )
    grid = lax.broadcasted_iota(jnp.int32, (length, experts * capacity), 1)
    pick = weight = 0.0
    for k, one in enumerate(named):
        rank = jnp.sum(jnp.where(one, ranks, 0.0), axis=1, keepdims=True).astype(jnp.int32)
        hit = grid == (chosen[:, k : k + 1] ^ place_ref[0]) * capacity + rank
        pick = pick + jnp.where(hit, 1.0, 0.0)
        weight = weight + jnp.where(hit, share[:, k : k + 1], 0.0)
    pick_ref[...] = jnp.transpose(pick).astype(BF16)
    high = weight.astype(BF16)
    high_ref[...] = high
    low_ref[...] = (weight - high.astype(F32)).astype(BF16)


def route(place, chosen, score, experts, capacity):
    length = chosen.shape[0]
    weight = jax.ShapeDtypeStruct((length, experts * capacity), BF16)
    return pl.pallas_call(
        lambda *refs: route_kernel(experts, capacity, *refs),
        in_specs=[pl.BlockSpec(memory_space=pltpu.SMEM)] + vmem(2),
        out_specs=vmem(3),
        out_shape=[jax.ShapeDtypeStruct((experts * capacity, length), BF16), weight, weight],
        compiler_params=pltpu.CompilerParams(vmem_limit_bytes=8 * 2**20),
        name="route",
    )(place, chosen, score)


def pack_kernel(*refs):
    height = refs[0].shape[0]
    for i, ref in enumerate(refs[:-1]):
        refs[-1][i * height : (i + 1) * height] = ref[...]


def pack(parts):
    height, wide = parts[0].shape
    return pl.pallas_call(
        pack_kernel,
        in_specs=vmem(len(parts)),
        out_specs=vmem(1)[0],
        out_shape=jax.ShapeDtypeStruct((height * len(parts), wide), BF16),
        compiler_params=pltpu.CompilerParams(vmem_limit_bytes=4 * 2**20),
        name="pack",
    )(*parts)


def project_kernel(n_tp, *refs):
    mixed, exits = refs[:n_tp], refs[n_tp : 2 * n_tp]
    skip_ref, pick_ref, stream_ref, *rows = refs[2 * n_tp :]
    total = 0.0
    for k in range(n_tp):
        total = total + jnp.dot(mixed[k][...], exits[k][...], preferred_element_type=F32)
    stream = (skip_ref[...].astype(F32) + total.astype(BF16).astype(F32)).astype(BF16)
    stream_ref[...] = stream
    picked = jnp.dot(pick_ref[...], stream, preferred_element_type=F32).astype(BF16)
    height = rows[0].shape[0]
    for k, ref in enumerate(rows):
        ref[...] = picked[k * height : (k + 1) * height]


def project(mixed, exits, skip, pick, experts):
    length, d_local = skip.shape
    n_tp = len(mixed)
    return pl.pallas_call(
        lambda *refs: project_kernel(n_tp, *refs),
        in_specs=vmem(2 * n_tp + 2),
        out_specs=vmem(1 + experts),
        out_shape=[jax.ShapeDtypeStruct((length, d_local), BF16)]
        + [jax.ShapeDtypeStruct((pick.shape[0] // experts, d_local), BF16)] * experts,
        compiler_params=pltpu.CompilerParams(vmem_limit_bytes=12 * 2**20),
        name="project",
    )(*mixed, *exits, skip, pick)


def fold_kernel(pairs, *refs):
    outs = refs[2 * pairs :]
    share = len(outs) // pairs
    for i in range(pairs):
        total = (refs[i][...].astype(F32) + refs[pairs + i][...].astype(F32)).astype(BF16)
        height = outs[i * share].shape[0]
        for j in range(share):
            outs[i * share + j][...] = total[j * height : (j + 1) * height]


def fold(kept, moved, share):
    rows, wide = kept[0].shape
    return pl.pallas_call(
        lambda *refs: fold_kernel(len(kept), *refs),
        in_specs=vmem(2 * len(kept)),
        out_specs=vmem(len(kept) * share),
        out_shape=[jax.ShapeDtypeStruct((rows // share, wide), BF16)] * (len(kept) * share),
        compiler_params=pltpu.CompilerParams(vmem_limit_bytes=6 * 2**20),
        name="fold",
    )(*kept, *moved)


def combine_kernel(stream_ref, high_ref, low_ref, *refs):
    out_ref = refs[-1]
    total = stream_ref[...].astype(F32)
    back = jnp.concatenate([ref[...] for ref in refs[:-1]], axis=0)
    total = total + jnp.dot(high_ref[...], back, preferred_element_type=F32)
    total = total + jnp.dot(low_ref[...], back, preferred_element_type=F32)
    out_ref[...] = total.astype(BF16)


def combine(stream, high, low, back):
    return pl.pallas_call(
        combine_kernel,
        in_specs=vmem(3 + len(back)),
        out_specs=vmem(1)[0],
        out_shape=jax.ShapeDtypeStruct(stream.shape, BF16),
        compiler_params=pltpu.CompilerParams(vmem_limit_bytes=8 * 2**20),
        name="combine",
    )(stream, high, low, *back)


def ffn_kernel(n_tp, width, place_ref, *refs):
    pieces = refs[:n_tp]
    scale_ref, gate_ref, up_ref, down_ref = refs[n_tp : n_tp + 4]
    outs = refs[n_tp + 4 :]
    me = place_ref[1]
    d_local = pieces[0].shape[1]
    square = gate = up = 0.0
    for k in range(n_tp):
        rows = pieces[k][...].astype(F32)
        square = square + jnp.sum(rows * rows, axis=1, keepdims=True)
        place = pl.multiple_of((me ^ k) * d_local, d_local)
        scaled = (rows * scale_ref[me ^ k]).astype(BF16)
        gate = gate + jnp.dot(
            scaled, gate_ref[pl.ds(place, d_local), :], preferred_element_type=F32
        )
        up = up + jnp.dot(scaled, up_ref[pl.ds(place, d_local), :], preferred_element_type=F32)
    inv_rms = lax.rsqrt(square / width + EPS)
    gate = gate * inv_rms
    hidden = (gate * jax.nn.sigmoid(gate) * (up * inv_rms)).astype(BF16)
    for k in range(n_tp):
        place = pl.multiple_of((me ^ k) * d_local, d_local)
        outs[k][...] = jnp.dot(
            hidden, down_ref[:, pl.ds(place, d_local)], preferred_element_type=F32
        ).astype(BF16)


def load_kernel(*refs):
    half = len(refs) // 2
    sems = refs[-1]
    copies = [
        pltpu.make_async_copy(refs[i], refs[half + i], sems.at[i]) for i in range(half)
    ]
    for copy in copies:
        copy.start()
    for copy in copies:
        copy.wait()


def load(*weights):
    return pl.pallas_call(
        load_kernel,
        in_specs=hbm(len(weights)),
        out_specs=vmem(len(weights)),
        out_shape=[jax.ShapeDtypeStruct(w.shape, w.dtype) for w in weights],
        scratch_shapes=[pltpu.SemaphoreType.DMA((len(weights),))],
        compiler_params=pltpu.CompilerParams(vmem_limit_bytes=16 * 2**20),
        name="load",
    )(*weights)


def ffn(place, pieces, scale, gate_w, up_w, down_w):
    n_tp = len(pieces)
    rows, d_local = pieces[0].shape
    width, units = gate_w.shape
    return pl.pallas_call(
        lambda *refs: ffn_kernel(n_tp, width, *refs),
        in_specs=[pl.BlockSpec(memory_space=pltpu.SMEM)] + vmem(n_tp + 4),
        out_specs=vmem(n_tp),
        out_shape=[jax.ShapeDtypeStruct((rows, d_local), BF16)] * n_tp,
        compiler_params=pltpu.CompilerParams(vmem_limit_bytes=24 * 2**20),
        cost_estimate=pl.CostEstimate(
            flops=6 * rows * width * units,
            bytes_accessed=6 * width * units + 4 * rows * width,
            transcendentals=rows * units,
        ),
        name="expert_ffn",
    )(place, *pieces, scale, gate_w, up_w, down_w)


def gather_pieces(own, n_tp):
    pieces = {0: own}
    bit = n_tp // 2
    while bit:
        for k in list(pieces):
            pieces[k ^ bit] = swap(pieces[k], "tp", bit)
        bit //= 2
    return [pieces[k] for k in range(n_tp)]


def scatter_sum(parts, n_tp, share):
    held = {k: parts[k] for k in range(n_tp)}
    bit = 1
    while bit < n_tp:
        sent = sorted((k for k in held if k & bit), reverse=True)
        moved = []
        for k in sent:
            moved.append(swap(held[k], "tp", bit))
        last = 2 * bit == n_tp
        sums = fold([held[k ^ bit] for k in sent], moved, share if last else 1)
        if last:
            return sums
        held = {k ^ bit: total for k, total in zip(sent, sums)}
        bit *= 2
    return [parts[0]]


def layer(
    lane_source_signal,
    spectral_damping_part,
    spectral_angular_part,
    interval_exponent,
    entry_matrix_inphase,
    entry_matrix_quadrature,
    emission_inphase,
    emission_quadrature,
    lane_bypass_factor,
    spike_shrink_offset,
    lane_exit_matrix,
    skipline_stream,
    specialist_scaling_vector,
    selected_specialists,
    dispatcher_scores,
    specialist_valve_matrix,
    specialist_widen_matrix,
    specialist_shrink_matrix,
):
    n_tp, experts = lax.axis_size("tp"), lax.axis_size("sp")
    d_local = specialist_scaling_vector.shape[0] // n_tp
    tok_local, top = selected_specialists.shape
    capacity = 2 * tok_local * top // experts
    place = jnp.stack([lax.axis_index("sp"), lax.axis_index("tp")]).astype(jnp.int32)
    exits, own_skip = cut_blocks(place, lane_exit_matrix, skipline_stream, n_tp)
    for k in range(1, n_tp):
        exits[k] = swap(exits[k], "tp", k)

    mixed = mixer(
        place,
        lane_source_signal,
        spectral_damping_part,
        spectral_angular_part,
        interval_exponent,
        entry_matrix_inphase,
        entry_matrix_quadrature,
        emission_inphase,
        emission_quadrature,
        lane_bypass_factor,
        spike_shrink_offset,
    )
    others = [mixed]
    for k in range(1, n_tp):
        others.append(swap(mixed, "tp", k))
    pick, high, low = route(place, selected_specialists, dispatcher_scores, experts, capacity)
    gate_w, up_w, down_w = load(
        specialist_valve_matrix[0], specialist_widen_matrix[0], specialist_shrink_matrix[0]
    )
    scale = specialist_scaling_vector.reshape(n_tp, 1, d_local)

    stream, *rows = project(others, exits, own_skip, pick, experts)
    arrived = {}
    for k in range(experts):
        arrived[k] = swap(rows[k], "sp", k) if k else rows[k]
    back = {}
    for chunk in chunks_of(experts):
        pieces = gather_pieces(pack([arrived[k] for k in chunk]), n_tp)
        parts = ffn(place, pieces, scale, gate_w, up_w, down_w)
        sums = scatter_sum(parts, n_tp, len(chunk))
        for k, total in zip(chunk, sums):
            back[k] = swap(total, "sp", k) if k else total
    return combine(stream, high, low, [back[k] for k in range(experts)])


def chunks_of(experts):
    near = list(range(experts // 2))
    far = list(range(experts // 2, experts))
    return near, far[: experts // 4], far[experts // 4 :]


def solution(mesh):
    placed = (
        P("tp", "sp"),
        P("tp", None),
        P("tp", None),
        P("tp"),
        P("tp", None, None),
        P("tp", None, None),
        P("tp", None, None),
        P("tp", None, None),
        P("tp"),
        P("tp", "sp"),
        P("tp", None),
        P("sp", None),
        P(),
        P("sp", None),
        P("sp", None),
        P("sp", None, "tp"),
        P("sp", None, "tp"),
        P("sp", "tp", None),
    )
    return jax.shard_map(
        layer, mesh=mesh, in_specs=placed, out_specs=P("sp", "tp"), check_vma=False
    )
```

```python
import jax
import jax.numpy as jnp
from jax import lax
from jax.experimental import pallas as pl
from jax.experimental.pallas import tpu as pltpu
from jax.sharding import PartitionSpec as P

EPS = 1e-06
F32 = jnp.float32
BF16 = jnp.bfloat16


def swap(value, axis, bits):
    count = lax.axis_size(axis)
    return lax.ppermute(value, axis, [(i, i ^ bits) for i in range(count)])


def expanded(columns, wide):
    return jnp.concatenate(
        [
            jnp.broadcast_to(columns[:, g : g + 1], (columns.shape[0], wide))
            for g in range(columns.shape[1])
        ],
        axis=1,
    )


def later(value, offset):
    if offset % 8:
        return pltpu.roll(value, offset, axis=0)
    return jnp.concatenate([value[-offset:], value[:-offset]], axis=0)


def block_rows(matrix, copies, inner):
    _, wide = matrix.shape
    spread = (
        lax.broadcasted_iota(jnp.int32, (wide, copies * wide), 1) % wide
        == lax.broadcasted_iota(jnp.int32, (wide, copies * wide), 0)
    ).astype(BF16)
    tiled = jnp.dot(matrix.astype(BF16), spread, preferred_element_type=F32)
    keep = (
        lax.broadcasted_iota(jnp.int32, tiled.shape, 0) // inner
        == lax.broadcasted_iota(jnp.int32, tiled.shape, 1) // wide
    )
    return jnp.where(keep, tiled, 0.0).astype(BF16)


def across(left, right):
    return lax.dot_general(left, right, (((1,), (1,)), ((), ())), preferred_element_type=F32)


def scan_kernel(
    signal_ref, damp_ref, turn_ref, pace_ref, ent_re_ref, ent_im_ref, shrink_ref,
    emit_re_ref, emit_im_ref, bypass_ref,
    summary_ref, local_ref, powers_ref, gone_ref,
):
    groups, states = damp_ref.shape
    length = shrink_ref.shape[1]
    lanes = ent_re_ref.shape[1]
    total = groups * states
    square = (groups, groups)
    step = jnp.where(
        lax.broadcasted_iota(jnp.int32, square, 0) == lax.broadcasted_iota(jnp.int32, square, 1),
        jnp.broadcast_to(pace_ref[...], square),
        0.0,
    )
    step = jnp.exp(jnp.sum(step, axis=1, keepdims=True))
    damp, turn = damp_ref[...], turn_ref[...]
    rate, angle = damp * step, turn * step
    size, cosine, sine = jnp.exp(rate), jnp.cos(angle), jnp.sin(angle)
    half = jnp.sin(0.5 * angle)
    series = rate * (1.0 + rate * 0.5 * (1.0 + rate * (1.0 / 3.0) * (1.0 + rate * 0.25)))
    less_one = jnp.where(jnp.abs(rate) < 0.05, series, size - 1.0)
    num_re = less_one * cosine - 2.0 * half * half
    num_im = size * sine
    denom = damp * damp + turn * turn
    own_group = (
        lax.broadcasted_iota(jnp.int32, (groups, total), 1) // states
        == lax.broadcasted_iota(jnp.int32, (groups, total), 0)
    )

    def row(value):
        spread = jnp.concatenate([value] * groups, axis=1)
        return jnp.sum(jnp.where(own_group, spread, 0.0), axis=0, keepdims=True)

    fac_re = row((num_re * damp + num_im * turn) / denom)
    fac_im = row((num_im * damp - num_re * turn) / denom)
    pow_re, pow_im = [row(size * cosine)], [row(num_im)]
    while 2 ** len(pow_re) < length:
        re, im = pow_re[-1], pow_im[-1]
        pow_re.append(re * re - im * im)
        pow_im.append(2.0 * re * im)
    for i, value in enumerate(pow_re + pow_im):
        powers_ref[i : i + 1, :] = value
    last = pow_re[-1], pow_im[-1]
    full_re = last[0] * last[0] - last[1] * last[1]
    full_im = 2.0 * last[0] * last[1]

    shrink = shrink_ref[...]
    summed = shrink
    position = lax.broadcasted_iota(jnp.int32, shrink.shape, 1)
    offset = 1
    while offset < length:
        summed = summed + jnp.where(
            position >= offset, pltpu.roll(summed, offset, axis=1), 0.0
        )
        offset *= 2
    columns = jnp.transpose(jnp.exp(jnp.concatenate([shrink, summed], axis=0)))
    gone_ref[...] = columns[:, groups:]
    all_gone = expanded(columns[length - 8 :, groups:], states)[7:8]
    flipped = jnp.transpose(signal_ref[...].astype(F32))
    local = bypass_ref[...] * flipped
    flipped = flipped.astype(BF16)
    ent_re = block_rows(ent_re_ref[...].reshape(groups * lanes, states), groups, lanes)
    ent_im = block_rows(ent_im_ref[...].reshape(groups * lanes, states), groups, lanes)
    emit_re = block_rows(emit_re_ref[...].reshape(groups * lanes, states), groups, lanes)
    emit_im = block_rows(emit_im_ref[...].reshape(groups * lanes, states), groups, lanes)
    wide = min(128, total)
    time = lax.broadcasted_iota(jnp.int32, (length, wide), 0)
    each = wide // states
    xs_re, xs_im = [], []
    for block in range(total // wide):
        cut = slice(block * wide, (block + 1) * wide)
        raw_re = jnp.dot(flipped, ent_re[:, cut], preferred_element_type=F32)
        raw_im = jnp.dot(flipped, ent_im[:, cut], preferred_element_type=F32)
        f_re, f_im = fac_re[:, cut], fac_im[:, cut]
        x_re = f_re * raw_re - f_im * raw_im
        x_im = f_re * raw_im + f_im * raw_re
        first = block * each
        decay = expanded(columns[:, first : first + each], states)
        decay = jnp.where(time >= 1, decay, 0.0)
        offset = 1
        for p_re, p_im in zip(pow_re, pow_im):
            a_re, a_im = p_re[:, cut], p_im[:, cut]
            s_re, s_im = later(x_re, offset), later(x_im, offset)
            x_re = x_re + decay * (a_re * s_re - a_im * s_im)
            x_im = x_im + decay * (a_re * s_im + a_im * s_re)
            if 2 * offset < length:
                decay = decay * later(decay, offset)
            offset *= 2
        local = local + across(x_re.astype(BF16), emit_re[:, cut])
        local = local - across(x_im.astype(BF16), emit_im[:, cut])
        xs_re.append(x_re[length - 8 :])
        xs_im.append(x_im[length - 8 :])
    local_ref[...] = local
    ends = []
    for value in (
        full_re * all_gone,
        full_im * all_gone,
        jnp.concatenate(xs_re, axis=1)[7:8],
        jnp.concatenate(xs_im, axis=1)[7:8],
    ):
        ends += [value[:, : total // 2], value[:, total // 2 :]]
    ends = jnp.concatenate(ends, axis=0)
    for s in range(summary_ref.shape[0]):
        summary_ref[s] = ends


def readout_kernel(
    mine_ref, pieces_ref, local_ref, powers_ref, gone_ref, emit_re_ref, emit_im_ref, mixed_ref
):
    groups, lanes, states = emit_re_ref.shape
    length, total = local_ref.shape[0], powers_ref.shape[1]
    mine = mine_ref[0]
    re = jnp.zeros((2, pieces_ref.shape[2]), F32)
    im = re
    for s in range(pieces_ref.shape[0] - 1):
        piece = pieces_ref[s]
        m_re, m_im, a_re, a_im = piece[0:2], piece[2:4], piece[4:6], piece[6:8]
        new_re = m_re * re - m_im * im + a_re
        new_im = m_re * im + m_im * re + a_im
        re = jnp.where(s < mine, new_re, re)
        im = jnp.where(s < mine, new_im, im)
    re = jnp.concatenate([re[0:1], re[1:2]], axis=1)
    im = jnp.concatenate([im[0:1], im[1:2]], axis=1)
    emit_re = block_rows(emit_re_ref[...].reshape(groups * lanes, states), groups, lanes)
    emit_im = block_rows(emit_im_ref[...].reshape(groups * lanes, states), groups, lanes)
    value = local_ref[...]
    bits = powers_ref.shape[0] // 2
    wide = min(128, total)
    each = wide // states
    near = lax.broadcasted_iota(jnp.int32, (8, wide), 0) + 1
    for block in range(total // wide):
        cut = slice(block * wide, (block + 1) * wide)
        p_re = [powers_ref[i : i + 1, cut] for i in range(bits)]
        p_im = [powers_ref[bits + i : bits + i + 1, cut] for i in range(bits)]
        c_re = jnp.broadcast_to(re[:, cut], (8, wide))
        c_im = jnp.broadcast_to(im[:, cut], (8, wide))
        for bit in range(4):
            a_re, a_im = p_re[bit], p_im[bit]
            on = (near >> bit) & 1 == 1
            c_re, c_im = (
                jnp.where(on, c_re * a_re - c_im * a_im, c_re),
                jnp.where(on, c_re * a_im + c_im * a_re, c_im),
            )
        bit = 3
        while c_re.shape[0] < length:
            a_re, a_im = p_re[bit], p_im[bit]
            c_re, c_im = (
                jnp.concatenate([c_re, c_re * a_re - c_im * a_im], axis=0),
                jnp.concatenate([c_im, c_re * a_im + c_im * a_re], axis=0),
            )
            bit += 1
        gone = expanded(gone_ref[:, block * each : (block + 1) * each], states)
        value = value + across((c_re * gone).astype(BF16), emit_re[:, cut])
        value = value - across((c_im * gone).astype(BF16), emit_im[:, cut])
    mixed_ref[...] = jax.nn.gelu(value).astype(BF16)


def vmem(count):
    return [pl.BlockSpec(memory_space=pltpu.VMEM)] * count


def hbm(count):
    return [pl.BlockSpec(memory_space=pltpu.HBM)] * count


def in_hbm(args):
    return [pltpu.with_memory_space_constraint(arg, pltpu.HBM) for arg in args]


def staged(kernel, first, count):
    def run(*refs):
        sources, buffers, sems = refs[first : first + count], refs[-count - 1 : -1], refs[-1]
        copies = [
            pltpu.make_async_copy(source, buffer, sems.at[i])
            for i, (source, buffer) in enumerate(zip(sources, buffers))
        ]
        for copy in copies:
            copy.start()
        for copy in copies:
            copy.wait()
        kernel(*refs[:first], *buffers, *refs[first + count : -count - 1])

    return run


def stage(args):
    return [pltpu.VMEM(arg.shape, arg.dtype) for arg in args] + [
        pltpu.SemaphoreType.DMA((len(args),))
    ]


def mixer_args(signal, damp, turn, pace, ent_re, ent_im, emit_re, emit_im, bypass, shrink):
    return (
        signal, damp, turn, pace.reshape(1, -1), ent_re.transpose(0, 2, 1),
        ent_im.transpose(0, 2, 1), shrink, bypass.reshape(1, -1), emit_re, emit_im,
    )


def first_kernel(*refs):
    sources, outs, buffers, sems = refs[:10], refs[10:16], refs[16:24], refs[24]
    for copy in run_copies([*zip(sources[:8], buffers), *zip(sources[8:], outs[4:])], sems):
        copy.wait()
    scan_kernel(*buffers[:7], *outs[4:6], buffers[7], *outs[:4])


def mixer(place, args):
    signal, damp, emit = args[0], args[1], args[8]
    groups, states = damp.shape
    channels, length = signal.shape
    total = groups * states
    count = lax.axis_size("sp")
    bits = (length - 1).bit_length()
    summary, local, powers, gone, emit_re, emit_im = pl.pallas_call(
        first_kernel,
        in_specs=hbm(10),
        out_specs=vmem(6),
        out_shape=[
            jax.ShapeDtypeStruct((count, 8, total // 2), F32),
            jax.ShapeDtypeStruct((length, channels), F32),
            jax.ShapeDtypeStruct((2 * bits, total), F32),
            jax.ShapeDtypeStruct((length, groups), F32),
            jax.ShapeDtypeStruct(emit.shape, F32),
            jax.ShapeDtypeStruct(emit.shape, F32),
        ],
        scratch_shapes=[pltpu.VMEM(arg.shape, arg.dtype) for arg in args[:8]]
        + [pltpu.SemaphoreType.DMA((10,))],
        compiler_params=pltpu.CompilerParams(vmem_limit_bytes=16 * 2**20),
        name="mixer_scan",
    )(*in_hbm(args))
    pieces = lax.all_to_all(summary, "sp", 0, 0, tiled=True)
    return pl.pallas_call(
        readout_kernel,
        in_specs=[pl.BlockSpec(memory_space=pltpu.SMEM)] + vmem(6),
        out_specs=vmem(1)[0],
        out_shape=jax.ShapeDtypeStruct((length, channels), BF16),
        compiler_params=pltpu.CompilerParams(vmem_limit_bytes=16 * 2**20),
        name="mixer_readout",
    )(place, pieces, local, powers, gone, emit_re, emit_im)


def block_of(ref, place_ref, k, wide):
    return ref.at[:, pl.ds(pl.multiple_of((place_ref[1] ^ k) * wide, wide), wide)]


def run_copies(pairs, sems):
    copies = [
        pltpu.make_async_copy(source, target, sems.at[i])
        for i, (source, target) in enumerate(pairs)
    ]
    for copy in copies:
        copy.start()
    return copies


def cut_kernel(n_tp, place_ref, exit_ref, skip_ref, *refs):
    evens, odd_ref, skip_out, sems = refs[: n_tp // 2], refs[-3], refs[-2], refs[-1]
    wide = skip_out.shape[1]
    pairs = []
    for i, ref in enumerate(evens):
        target = odd_ref.at[:, i * wide : (i + 1) * wide]
        pairs.append((block_of(exit_ref, place_ref, 2 * i + 1, wide), target))
        pairs.append((block_of(exit_ref, place_ref, 2 * i, wide), ref))
    pairs.append((block_of(skip_ref, place_ref, 0, wide), skip_out))
    for copy in run_copies(pairs, sems):
        copy.wait()


def cut_blocks(place, exit_matrix, skip, n_tp):
    channels, wide = exit_matrix.shape[0], exit_matrix.shape[1] // n_tp
    *evens, odd, own_skip = pl.pallas_call(
        lambda *refs: cut_kernel(n_tp, *refs),
        in_specs=[pl.BlockSpec(memory_space=pltpu.SMEM)] + hbm(2),
        out_specs=vmem(n_tp // 2 + 2),
        out_shape=[jax.ShapeDtypeStruct((channels, wide), BF16)] * (n_tp // 2)
        + [
            jax.ShapeDtypeStruct((channels, wide * n_tp // 2), BF16),
            jax.ShapeDtypeStruct((skip.shape[0], wide), BF16),
        ],
        scratch_shapes=[pltpu.SemaphoreType.DMA((n_tp + 1,))],
        compiler_params=pltpu.CompilerParams(vmem_limit_bytes=4 * 2**20),
        name="cut_blocks",
    )(place, *in_hbm((exit_matrix, skip)))
    return evens, odd, own_skip


def partial_kernel(mixed_ref, other_ref, odd_ref, *refs):
    evens, outs = refs[: len(refs) // 2], refs[len(refs) // 2 :]
    wide = evens[0].shape[1]
    for i, (even, out) in enumerate(zip(evens, outs)):
        total = jnp.dot(mixed_ref[...], even[...], preferred_element_type=F32)
        total = total + jnp.dot(
            other_ref[...], odd_ref[:, i * wide : (i + 1) * wide], preferred_element_type=F32
        )
        out[...] = total.astype(out.dtype)


def partial_sums(mixed, other, odd, evens):
    length, wide = mixed.shape[0], evens[0].shape[1]
    kinds = [F32] + [BF16] * (len(evens) - 1)
    return pl.pallas_call(
        partial_kernel,
        in_specs=vmem(3 + len(evens)),
        out_specs=vmem(len(evens)),
        out_shape=[jax.ShapeDtypeStruct((length, wide), kind) for kind in kinds],
        compiler_params=pltpu.CompilerParams(vmem_limit_bytes=8 * 2**20),
        name="partial_sums",
    )(mixed, other, odd, *evens)


def route_kernel(experts, capacity, place_ref, chosen_ref, score_ref, pick_ref, high_ref, low_ref):
    top, length = chosen_ref.shape
    square = (length, length)
    diagonal = (
        lax.broadcasted_iota(jnp.int32, square, 0) == lax.broadcasted_iota(jnp.int32, square, 1)
    )

    def column(row):
        spread = jnp.where(diagonal, jnp.broadcast_to(row, square), 0.0)
        return jnp.sum(spread, axis=1, keepdims=True)

    score = [column(score_ref[k : k + 1, :]) for k in range(top)]
    chosen = [
        column(chosen_ref[k : k + 1, :].astype(F32)).astype(jnp.int32) for k in range(top)
    ]
    whole = sum(score)
    lane = lax.broadcasted_iota(jnp.int32, (length, experts), 1)
    named = [chosen[k] == lane for k in range(top)]
    counted = sum(jnp.where(one, 1.0, 0.0) for one in named)
    before = (
        lax.broadcasted_iota(jnp.int32, (length, length), 0)
        > lax.broadcasted_iota(jnp.int32, (length, length), 1)
    )
    ranks = jnp.dot(
        jnp.where(before, 1.0, 0.0).astype(BF16), counted.astype(BF16),
        preferred_element_type=F32,
    )
    grid = lax.broadcasted_iota(jnp.int32, (length, experts * capacity), 1)
    pick = weight = 0.0
    for k, one in enumerate(named):
        rank = jnp.sum(jnp.where(one, ranks, 0.0), axis=1, keepdims=True).astype(jnp.int32)
        hit = grid == (chosen[k] ^ place_ref[0]) * capacity + rank
        pick = pick + jnp.where(hit, 1.0, 0.0)
        weight = weight + jnp.where(hit, score[k] / whole, 0.0)
    pick_ref[...] = jnp.transpose(pick).astype(BF16)
    high = weight.astype(BF16)
    high_ref[...] = high
    low_ref[...] = (weight - high.astype(F32)).astype(BF16)


def route(place, chosen, score, experts, capacity):
    length = chosen.shape[0]
    weight = jax.ShapeDtypeStruct((length, experts * capacity), BF16)
    args = (chosen.T, score.T)
    return pl.pallas_call(
        staged(lambda *refs: route_kernel(experts, capacity, *refs), 1, len(args)),
        in_specs=[pl.BlockSpec(memory_space=pltpu.SMEM)] + hbm(2),
        out_specs=vmem(3),
        scratch_shapes=stage(args),
        out_shape=[jax.ShapeDtypeStruct((experts * capacity, length), BF16), weight, weight],
        compiler_params=pltpu.CompilerParams(vmem_limit_bytes=8 * 2**20),
        name="route",
    )(place, *in_hbm(args))


def pack_kernel(*refs):
    height = refs[0].shape[0]
    for i, ref in enumerate(refs[:-1]):
        refs[-1][i * height : (i + 1) * height] = ref[...]


def pack(parts):
    height, wide = parts[0].shape
    return pl.pallas_call(
        pack_kernel,
        in_specs=vmem(len(parts)),
        out_specs=vmem(1)[0],
        out_shape=jax.ShapeDtypeStruct((height * len(parts), wide), BF16),
        compiler_params=pltpu.CompilerParams(vmem_limit_bytes=4 * 2**20),
        name="pack",
    )(*parts)


def project_kernel(count, *refs):
    skip_ref, pick_ref, stream_ref, *rows = refs[count:]
    total = refs[0][...]
    for ref in refs[1:count]:
        total = total + ref[...].astype(F32)
    stream = (skip_ref[...].astype(F32) + total.astype(BF16).astype(F32)).astype(BF16)
    stream_ref[...] = stream
    picked = jnp.dot(pick_ref[...], stream, preferred_element_type=F32).astype(BF16)
    height = rows[0].shape[0]
    for k, ref in enumerate(rows):
        ref[...] = picked[k * height : (k + 1) * height]


def project(sums, skip, pick, experts):
    length, d_local = skip.shape
    return pl.pallas_call(
        lambda *refs: project_kernel(len(sums), *refs),
        in_specs=vmem(len(sums) + 2),
        out_specs=vmem(1 + experts),
        out_shape=[jax.ShapeDtypeStruct((length, d_local), BF16)]
        + [jax.ShapeDtypeStruct((pick.shape[0] // experts, d_local), BF16)] * experts,
        compiler_params=pltpu.CompilerParams(vmem_limit_bytes=8 * 2**20),
        name="project",
    )(*sums, skip, pick)


def fold_kernel(pairs, *refs):
    outs = refs[2 * pairs :]
    share = len(outs) // pairs
    for i in range(pairs):
        total = (refs[i][...].astype(F32) + refs[pairs + i][...].astype(F32)).astype(BF16)
        height = outs[i * share].shape[0]
        for j in range(share):
            outs[i * share + j][...] = total[j * height : (j + 1) * height]


def fold(kept, moved, share):
    rows, wide = kept[0].shape
    return pl.pallas_call(
        lambda *refs: fold_kernel(len(kept), *refs),
        in_specs=vmem(2 * len(kept)),
        out_specs=vmem(len(kept) * share),
        out_shape=[jax.ShapeDtypeStruct((rows // share, wide), BF16)] * (len(kept) * share),
        compiler_params=pltpu.CompilerParams(vmem_limit_bytes=6 * 2**20),
        name="fold",
    )(*kept, *moved)


def combine_kernel(stream_ref, high_ref, low_ref, *refs):
    out_ref = refs[-1]
    total = stream_ref[...].astype(F32)
    back = jnp.concatenate([ref[...] for ref in refs[:-1]], axis=0)
    total = total + jnp.dot(high_ref[...], back, preferred_element_type=F32)
    total = total + jnp.dot(low_ref[...], back, preferred_element_type=F32)
    out_ref[...] = total.astype(BF16)


def combine(stream, high, low, back):
    return pl.pallas_call(
        combine_kernel,
        in_specs=vmem(3 + len(back)),
        out_specs=vmem(1)[0],
        out_shape=jax.ShapeDtypeStruct(stream.shape, BF16),
        compiler_params=pltpu.CompilerParams(vmem_limit_bytes=8 * 2**20),
        name="combine",
    )(stream, high, low, *back)


def ffn_kernel(n_tp, groups, width, place_ref, *refs):
    pieces = refs[: n_tp * groups]
    scale_ref, gate_ref, up_ref, down_ref = refs[n_tp * groups : n_tp * groups + 4]
    outs = refs[n_tp * groups + 4 :]
    me = place_ref[1]
    d_local = pieces[0].shape[1]
    square = gate = up = 0.0
    for k in range(n_tp):
        parts = [pieces[g * n_tp + k][...] for g in range(groups)]
        rows = jnp.concatenate(parts, axis=0).astype(F32)
        square = square + jnp.sum(rows * rows, axis=1, keepdims=True)
        place = pl.multiple_of((me ^ k) * d_local, d_local)
        scaled = (rows * scale_ref[me ^ k]).astype(BF16)
        gate = gate + jnp.dot(
            scaled, gate_ref[pl.ds(place, d_local), :], preferred_element_type=F32
        )
        up = up + jnp.dot(scaled, up_ref[pl.ds(place, d_local), :], preferred_element_type=F32)
    inv_rms = lax.rsqrt(square / width + EPS)
    gate = gate * inv_rms
    hidden = (gate * jax.nn.sigmoid(gate) * (up * inv_rms)).astype(BF16)
    for k in range(n_tp):
        place = pl.multiple_of((me ^ k) * d_local, d_local)
        done = jnp.dot(
            hidden, down_ref[:, pl.ds(place, d_local)], preferred_element_type=F32
        ).astype(BF16)
        start = 0
        for g in range(groups):
            out = outs[g * n_tp + k]
            out[...] = done[start : start + out.shape[0]]
            start += out.shape[0]


def load_kernel(*refs):
    half = len(refs) // 2
    sems = refs[-1]
    copies = [
        pltpu.make_async_copy(refs[i], refs[half + i], sems.at[i]) for i in range(half)
    ]
    for copy in copies:
        copy.start()
    for copy in copies:
        copy.wait()


def load(*weights):
    return pl.pallas_call(
        load_kernel,
        in_specs=hbm(len(weights)),
        out_specs=vmem(len(weights)),
        out_shape=[jax.ShapeDtypeStruct(w.shape, w.dtype) for w in weights],
        scratch_shapes=[pltpu.SemaphoreType.DMA((len(weights),))],
        compiler_params=pltpu.CompilerParams(vmem_limit_bytes=16 * 2**20),
        name="load",
    )(*in_hbm(weights))


def ffn(place, grouped, scale, gate_w, up_w, down_w):
    n_tp, groups = len(grouped[0]), len(grouped)
    pieces = [piece for group in grouped for piece in group]
    rows = sum(group[0].shape[0] for group in grouped)
    width, units = gate_w.shape
    outs = pl.pallas_call(
        lambda *refs: ffn_kernel(n_tp, groups, width, *refs),
        in_specs=[pl.BlockSpec(memory_space=pltpu.SMEM)] + vmem(len(pieces) + 4),
        out_specs=vmem(len(pieces)),
        out_shape=[jax.ShapeDtypeStruct(piece.shape, BF16) for piece in pieces],
        compiler_params=pltpu.CompilerParams(vmem_limit_bytes=24 * 2**20),
        cost_estimate=pl.CostEstimate(
            flops=6 * rows * width * units,
            bytes_accessed=6 * width * units + 4 * rows * width,
            transcendentals=rows * units,
        ),
        name="expert_ffn",
    )(place, *pieces, scale, gate_w, up_w, down_w)
    return [outs[g * n_tp : (g + 1) * n_tp] for g in range(groups)]


def gather_pieces(own, n_tp):
    pieces = {0: own}
    bit = n_tp // 2
    while bit:
        for k in list(pieces):
            pieces[k ^ bit] = swap(pieces[k], "tp", bit)
        bit //= 2
    return [pieces[k] for k in range(n_tp)]


def scatter_sum(parts, n_tp, share):
    held = {k: parts[k] for k in range(n_tp)}
    bit = 1
    while bit < n_tp:
        sent = sorted((k for k in held if k & bit), reverse=True)
        moved = []
        for k in sent:
            moved.append(swap(held[k], "tp", bit))
        last = 2 * bit == n_tp
        sums = fold([held[k ^ bit] for k in sent], moved, share if last else 1)
        if last:
            return sums
        held = {k ^ bit: total for k, total in zip(sent, sums)}
        bit *= 2
    return [parts[0]]


def layer(
    lane_source_signal,
    spectral_damping_part,
    spectral_angular_part,
    interval_exponent,
    entry_matrix_inphase,
    entry_matrix_quadrature,
    emission_inphase,
    emission_quadrature,
    lane_bypass_factor,
    spike_shrink_offset,
    lane_exit_matrix,
    skipline_stream,
    specialist_scaling_vector,
    selected_specialists,
    dispatcher_scores,
    specialist_valve_matrix,
    specialist_widen_matrix,
    specialist_shrink_matrix,
):
    n_tp, experts = lax.axis_size("tp"), lax.axis_size("sp")
    d_local = specialist_scaling_vector.shape[0] // n_tp
    tok_local, top = selected_specialists.shape
    capacity = 2 * tok_local * top // experts
    place = jnp.stack([lax.axis_index("sp"), lax.axis_index("tp")]).astype(jnp.int32)
    args = mixer_args(
        lane_source_signal,
        spectral_damping_part,
        spectral_angular_part,
        interval_exponent,
        entry_matrix_inphase,
        entry_matrix_quadrature,
        emission_inphase,
        emission_quadrature,
        lane_bypass_factor,
        spike_shrink_offset,
    )
    evens, odd, own_skip = cut_blocks(place, lane_exit_matrix, skipline_stream, n_tp)
    odd = swap(odd, "tp", 1)
    mixed = mixer(place, args)
    other = swap(mixed, "tp", 1)
    held = dict(zip(range(0, n_tp, 2), partial_sums(mixed, other, odd, evens)))
    sums = [held[0]]
    bit = 2
    while bit < n_tp:
        for k in [k for k in held if k & bit]:
            moved = swap(held.pop(k), "tp", bit)
            if k == bit:
                sums.append(moved)
            else:
                held[k ^ bit] = (held[k ^ bit].astype(F32) + moved.astype(F32)).astype(BF16)
        bit *= 2
    pick, high, low = route(place, selected_specialists, dispatcher_scores, experts, capacity)
    gate_w, up_w = load(specialist_valve_matrix[0], specialist_widen_matrix[0])
    (down_w,) = load(specialist_shrink_matrix[0])
    scale = specialist_scaling_vector.reshape(n_tp, 1, d_local)

    stream, *rows = project(sums, own_skip, pick, experts)
    arrived = {}
    for k in range(experts):
        arrived[k] = swap(rows[k], "sp", k) if k else rows[k]
    chunks = chunks_of(experts)
    pieces = []
    for chunk in chunks:
        own = [arrived[k] for k in chunk]
        pieces.append(gather_pieces(pack(own) if len(own) > 1 else own[0], n_tp))
    parts = []
    for members in calls_of(len(chunks)):
        parts += ffn(place, [pieces[i] for i in members], scale, gate_w, up_w, down_w)
    back = {}
    for c, chunk in enumerate(chunks):
        sums = scatter_sum(parts[c], n_tp, len(chunk))
        for k, total in zip(chunk, sums):
            back[k] = swap(total, "sp", k) if k else total
    return combine(stream, high, low, [back[k] for k in range(experts)])


def chunks_of(experts):
    half, part = experts // 2, experts // 4
    cuts = [0, max(1, experts // 8), half, half + part, experts]
    return [list(range(a, b)) for a, b in zip(cuts, cuts[1:])]


def calls_of(chunks):
    return [(0, 1)] + [(c,) for c in range(2, chunks)]


def solution(mesh):
    placed = (
        P("tp", "sp"),
        P("tp", None),
        P("tp", None),
        P("tp"),
        P("tp", None, None),
        P("tp", None, None),
        P("tp", None, None),
        P("tp", None, None),
        P("tp"),
        P("tp", "sp"),
        P("tp", None),
        P("sp", None),
        P(),
        P("sp", None),
        P("sp", None),
        P("sp", None, "tp"),
        P("sp", None, "tp"),
        P("sp", "tp", None),
    )
    return jax.shard_map(
        layer, mesh=mesh, in_specs=placed, out_specs=P("sp", "tp"), check_vma=False
    )
```

```python
import jax
import jax.numpy as jnp
from jax import lax
from jax.experimental import pallas as pl
from jax.experimental.pallas import tpu as pltpu
from jax.sharding import PartitionSpec as P

EPS = 1e-06
F32 = jnp.float32
BF16 = jnp.bfloat16


def swap(value, axis, bits):
    count = lax.axis_size(axis)
    return lax.ppermute(value, axis, [(i, i ^ bits) for i in range(count)])


def expanded(columns, wide):
    return jnp.concatenate(
        [
            jnp.broadcast_to(columns[:, g : g + 1], (columns.shape[0], wide))
            for g in range(columns.shape[1])
        ],
        axis=1,
    )


def later(value, offset):
    if offset % 8:
        return pltpu.roll(value, offset, axis=0)
    return jnp.concatenate([value[-offset:], value[:-offset]], axis=0)


def block_rows(matrix, copies, inner):
    _, wide = matrix.shape
    spread = (
        lax.broadcasted_iota(jnp.int32, (wide, copies * wide), 1) % wide
        == lax.broadcasted_iota(jnp.int32, (wide, copies * wide), 0)
    ).astype(BF16)
    tiled = jnp.dot(matrix.astype(BF16), spread, preferred_element_type=F32)
    keep = (
        lax.broadcasted_iota(jnp.int32, tiled.shape, 0) // inner
        == lax.broadcasted_iota(jnp.int32, tiled.shape, 1) // wide
    )
    return jnp.where(keep, tiled, 0.0).astype(BF16)


def across(left, right):
    return lax.dot_general(left, right, (((1,), (1,)), ((), ())), preferred_element_type=F32)


def scan_kernel(
    signal_ref, damp_ref, turn_ref, pace_ref, ent_re_ref, ent_im_ref, shrink_ref,
    emit_re_ref, emit_im_ref, bypass_ref,
    summary_ref, local_ref, powers_ref, gone_ref,
):
    groups, states = damp_ref.shape
    length = shrink_ref.shape[1]
    lanes = ent_re_ref.shape[1]
    total = groups * states
    square = (groups, groups)
    step = jnp.where(
        lax.broadcasted_iota(jnp.int32, square, 0) == lax.broadcasted_iota(jnp.int32, square, 1),
        jnp.broadcast_to(pace_ref[...], square),
        0.0,
    )
    step = jnp.exp(jnp.sum(step, axis=1, keepdims=True))
    damp, turn = damp_ref[...], turn_ref[...]
    rate, angle = damp * step, turn * step
    size, cosine, sine = jnp.exp(rate), jnp.cos(angle), jnp.sin(angle)
    half = jnp.sin(0.5 * angle)
    series = rate * (1.0 + rate * 0.5 * (1.0 + rate * (1.0 / 3.0) * (1.0 + rate * 0.25)))
    less_one = jnp.where(jnp.abs(rate) < 0.05, series, size - 1.0)
    num_re = less_one * cosine - 2.0 * half * half
    num_im = size * sine
    denom = damp * damp + turn * turn
    own_group = (
        lax.broadcasted_iota(jnp.int32, (groups, total), 1) // states
        == lax.broadcasted_iota(jnp.int32, (groups, total), 0)
    )

    def row(value):
        spread = jnp.concatenate([value] * groups, axis=1)
        return jnp.sum(jnp.where(own_group, spread, 0.0), axis=0, keepdims=True)

    fac_re = row((num_re * damp + num_im * turn) / denom)
    fac_im = row((num_im * damp - num_re * turn) / denom)
    pow_re, pow_im = [row(size * cosine)], [row(num_im)]
    while 2 ** len(pow_re) < length:
        re, im = pow_re[-1], pow_im[-1]
        pow_re.append(re * re - im * im)
        pow_im.append(2.0 * re * im)
    for i, value in enumerate(pow_re + pow_im):
        powers_ref[i : i + 1, :] = value

    shrink = shrink_ref[...]
    summed = shrink
    position = lax.broadcasted_iota(jnp.int32, shrink.shape, 1)
    offset = 1
    while offset < length:
        summed = summed + jnp.where(
            position >= offset, pltpu.roll(summed, offset, axis=1), 0.0
        )
        offset *= 2
    columns = jnp.transpose(jnp.exp(jnp.concatenate([shrink, summed], axis=0)))
    gone_ref[...] = columns[:, groups:]
    all_gone = columns[length - 8 :, groups:][7:8]
    flipped = jnp.transpose(signal_ref[...].astype(F32))
    local = bypass_ref[...] * flipped
    flipped = flipped.astype(BF16)
    ent_re = block_rows(ent_re_ref[...].reshape(groups * lanes, states), groups, lanes)
    ent_im = block_rows(ent_im_ref[...].reshape(groups * lanes, states), groups, lanes)
    emit_re = block_rows(emit_re_ref[...].reshape(groups * lanes, states), groups, lanes)
    emit_im = block_rows(emit_im_ref[...].reshape(groups * lanes, states), groups, lanes)
    wide = min(128, total)
    time = lax.broadcasted_iota(jnp.int32, (length, wide), 0)
    each = wide // states
    xs_re, xs_im = [], []
    for block in range(total // wide):
        cut = slice(block * wide, (block + 1) * wide)
        raw_re = jnp.dot(flipped, ent_re[:, cut], preferred_element_type=F32)
        raw_im = jnp.dot(flipped, ent_im[:, cut], preferred_element_type=F32)
        f_re, f_im = fac_re[:, cut], fac_im[:, cut]
        x_re = f_re * raw_re - f_im * raw_im
        x_im = f_re * raw_im + f_im * raw_re
        first = block * each
        decay = expanded(columns[:, first : first + each], states)
        decay = jnp.where(time >= 1, decay, 0.0)
        offset = 1
        for p_re, p_im in zip(pow_re, pow_im):
            a_re, a_im = p_re[:, cut], p_im[:, cut]
            s_re, s_im = later(x_re, offset), later(x_im, offset)
            x_re = x_re + decay * (a_re * s_re - a_im * s_im)
            x_im = x_im + decay * (a_re * s_im + a_im * s_re)
            if 2 * offset < length:
                decay = decay * later(decay, offset)
            offset *= 2
        local = local + across(x_re.astype(BF16), emit_re[:, cut])
        local = local - across(x_im.astype(BF16), emit_im[:, cut])
        xs_re.append(x_re[length - 8 :])
        xs_im.append(x_im[length - 8 :])
    local_ref[...] = local
    spare = summary_ref.shape[2] - 2 * total - groups
    ends = jnp.concatenate(
        [
            jnp.concatenate(xs_re, axis=1)[7:8],
            jnp.concatenate(xs_im, axis=1)[7:8],
            all_gone,
            jnp.zeros((1, spare), F32),
        ],
        axis=1,
    )
    for s in range(summary_ref.shape[0]):
        summary_ref[s] = ends


def readout_kernel(
    mine_ref, pieces_ref, local_ref, powers_ref, gone_ref, emit_re_ref, emit_im_ref, mixed_ref
):
    groups, lanes, states = emit_re_ref.shape
    length, total = local_ref.shape[0], powers_ref.shape[1]
    mine = mine_ref[0]
    bits = powers_ref.shape[0] // 2
    half_re, half_im = powers_ref[bits - 1 : bits, :], powers_ref[2 * bits - 1 : 2 * bits, :]
    full_re = half_re * half_re - half_im * half_im
    full_im = 2.0 * half_re * half_im
    re = jnp.zeros((1, total), F32)
    im = re
    for s in range(pieces_ref.shape[0] - 1):
        piece = pieces_ref[s]
        fade = expanded(piece[:, 2 * total : 2 * total + groups], states)
        m_re, m_im = full_re * fade, full_im * fade
        new_re = m_re * re - m_im * im + piece[:, :total]
        new_im = m_re * im + m_im * re + piece[:, total : 2 * total]
        re = jnp.where(s < mine, new_re, re)
        im = jnp.where(s < mine, new_im, im)
    emit_re = block_rows(emit_re_ref[...].reshape(groups * lanes, states), groups, lanes)
    emit_im = block_rows(emit_im_ref[...].reshape(groups * lanes, states), groups, lanes)
    value = local_ref[...]
    wide = min(128, total)
    each = wide // states
    near = lax.broadcasted_iota(jnp.int32, (8, wide), 0) + 1
    for block in range(total // wide):
        cut = slice(block * wide, (block + 1) * wide)
        p_re = [powers_ref[i : i + 1, cut] for i in range(bits)]
        p_im = [powers_ref[bits + i : bits + i + 1, cut] for i in range(bits)]
        c_re = jnp.broadcast_to(re[:, cut], (8, wide))
        c_im = jnp.broadcast_to(im[:, cut], (8, wide))
        for bit in range(4):
            a_re, a_im = p_re[bit], p_im[bit]
            on = (near >> bit) & 1 == 1
            c_re, c_im = (
                jnp.where(on, c_re * a_re - c_im * a_im, c_re),
                jnp.where(on, c_re * a_im + c_im * a_re, c_im),
            )
        bit = 3
        while c_re.shape[0] < length:
            a_re, a_im = p_re[bit], p_im[bit]
            c_re, c_im = (
                jnp.concatenate([c_re, c_re * a_re - c_im * a_im], axis=0),
                jnp.concatenate([c_im, c_re * a_im + c_im * a_re], axis=0),
            )
            bit += 1
        gone = expanded(gone_ref[:, block * each : (block + 1) * each], states)
        value = value + across((c_re * gone).astype(BF16), emit_re[:, cut])
        value = value - across((c_im * gone).astype(BF16), emit_im[:, cut])
    mixed_ref[...] = jax.nn.gelu(value).astype(BF16)


def vmem(count):
    return [pl.BlockSpec(memory_space=pltpu.VMEM)] * count


def hbm(count):
    return [pl.BlockSpec(memory_space=pltpu.HBM)] * count


def in_hbm(args):
    return [pltpu.with_memory_space_constraint(arg, pltpu.HBM) for arg in args]


def staged(kernel, first, count):
    def run(*refs):
        sources, buffers, sems = refs[first : first + count], refs[-count - 1 : -1], refs[-1]
        copies = [
            pltpu.make_async_copy(source, buffer, sems.at[i])
            for i, (source, buffer) in enumerate(zip(sources, buffers))
        ]
        for copy in copies:
            copy.start()
        for copy in copies:
            copy.wait()
        kernel(*refs[:first], *buffers, *refs[first + count : -count - 1])

    return run


def stage(args):
    return [pltpu.VMEM(arg.shape, arg.dtype) for arg in args] + [
        pltpu.SemaphoreType.DMA((len(args),))
    ]


def mixer_args(signal, damp, turn, pace, ent_re, ent_im, emit_re, emit_im, bypass, shrink):
    return (
        signal, damp, turn, pace.reshape(1, -1), ent_re.transpose(0, 2, 1),
        ent_im.transpose(0, 2, 1), shrink, bypass.reshape(1, -1), emit_re, emit_im,
    )


def first_kernel(*refs):
    sources, outs, buffers, sems = refs[:10], refs[10:16], refs[16:24], refs[24]
    for copy in run_copies([*zip(sources[:8], buffers), *zip(sources[8:], outs[4:])], sems):
        copy.wait()
    scan_kernel(*buffers[:7], *outs[4:6], buffers[7], *outs[:4])


def mixer(place, args):
    signal, damp, emit = args[0], args[1], args[8]
    groups, states = damp.shape
    channels, length = signal.shape
    total = groups * states
    count = lax.axis_size("sp")
    bits = (length - 1).bit_length()
    summary, local, powers, gone, emit_re, emit_im = pl.pallas_call(
        first_kernel,
        in_specs=hbm(10),
        out_specs=vmem(6),
        out_shape=[
            jax.ShapeDtypeStruct((count, 1, 2 * total + 128), F32),
            jax.ShapeDtypeStruct((length, channels), F32),
            jax.ShapeDtypeStruct((2 * bits, total), F32),
            jax.ShapeDtypeStruct((length, groups), F32),
            jax.ShapeDtypeStruct(emit.shape, F32),
            jax.ShapeDtypeStruct(emit.shape, F32),
        ],
        scratch_shapes=[pltpu.VMEM(arg.shape, arg.dtype) for arg in args[:8]]
        + [pltpu.SemaphoreType.DMA((10,))],
        compiler_params=pltpu.CompilerParams(vmem_limit_bytes=16 * 2**20),
        name="mixer_scan",
    )(*in_hbm(args))
    pieces = lax.all_to_all(summary, "sp", 0, 0, tiled=True)
    return pl.pallas_call(
        readout_kernel,
        in_specs=[pl.BlockSpec(memory_space=pltpu.SMEM)] + vmem(6),
        out_specs=vmem(1)[0],
        out_shape=jax.ShapeDtypeStruct((length, channels), BF16),
        compiler_params=pltpu.CompilerParams(vmem_limit_bytes=16 * 2**20),
        name="mixer_readout",
    )(place, pieces, local, powers, gone, emit_re, emit_im)


def block_of(ref, place_ref, k, wide):
    return ref.at[:, pl.ds(pl.multiple_of((place_ref[1] ^ k) * wide, wide), wide)]


def run_copies(pairs, sems):
    copies = [
        pltpu.make_async_copy(source, target, sems.at[i])
        for i, (source, target) in enumerate(pairs)
    ]
    for copy in copies:
        copy.start()
    return copies


def cut_kernel(n_tp, place_ref, exit_ref, skip_ref, *refs):
    evens, odd_ref, skip_out, sems = refs[: n_tp // 2], refs[-3], refs[-2], refs[-1]
    wide = skip_out.shape[1]
    pairs = []
    for i, ref in enumerate(evens):
        target = odd_ref.at[:, i * wide : (i + 1) * wide]
        pairs.append((block_of(exit_ref, place_ref, 2 * i + 1, wide), target))
        pairs.append((block_of(exit_ref, place_ref, 2 * i, wide), ref))
    pairs.append((block_of(skip_ref, place_ref, 0, wide), skip_out))
    for copy in run_copies(pairs, sems):
        copy.wait()


def cut_blocks(place, exit_matrix, skip, n_tp):
    channels, wide = exit_matrix.shape[0], exit_matrix.shape[1] // n_tp
    *evens, odd, own_skip = pl.pallas_call(
        lambda *refs: cut_kernel(n_tp, *refs),
        in_specs=[pl.BlockSpec(memory_space=pltpu.SMEM)] + hbm(2),
        out_specs=vmem(n_tp // 2 + 2),
        out_shape=[jax.ShapeDtypeStruct((channels, wide), BF16)] * (n_tp // 2)
        + [
            jax.ShapeDtypeStruct((channels, wide * n_tp // 2), BF16),
            jax.ShapeDtypeStruct((skip.shape[0], wide), BF16),
        ],
        scratch_shapes=[pltpu.SemaphoreType.DMA((n_tp + 1,))],
        compiler_params=pltpu.CompilerParams(vmem_limit_bytes=4 * 2**20),
        name="cut_blocks",
    )(place, *in_hbm((exit_matrix, skip)))
    return evens, odd, own_skip


def partial_kernel(mixed_ref, other_ref, odd_ref, *refs):
    evens, outs = refs[: len(refs) // 2], refs[len(refs) // 2 :]
    wide = evens[0].shape[1]
    for i, (even, out) in enumerate(zip(evens, outs)):
        total = jnp.dot(mixed_ref[...], even[...], preferred_element_type=F32)
        total = total + jnp.dot(
            other_ref[...], odd_ref[:, i * wide : (i + 1) * wide], preferred_element_type=F32
        )
        out[...] = total.astype(out.dtype)


def partial_sums(mixed, other, odd, evens):
    length, wide = mixed.shape[0], evens[0].shape[1]
    kinds = [F32] + [BF16] * (len(evens) - 1)
    return pl.pallas_call(
        partial_kernel,
        in_specs=vmem(3 + len(evens)),
        out_specs=vmem(len(evens)),
        out_shape=[jax.ShapeDtypeStruct((length, wide), kind) for kind in kinds],
        compiler_params=pltpu.CompilerParams(vmem_limit_bytes=8 * 2**20),
        name="partial_sums",
    )(mixed, other, odd, *evens)


def route_kernel(experts, capacity, place_ref, chosen_ref, score_ref, pick_ref, high_ref, low_ref):
    top, length = chosen_ref.shape
    square = (length, length)
    diagonal = (
        lax.broadcasted_iota(jnp.int32, square, 0) == lax.broadcasted_iota(jnp.int32, square, 1)
    )

    def column(row):
        spread = jnp.where(diagonal, jnp.broadcast_to(row, square), 0.0)
        return jnp.sum(spread, axis=1, keepdims=True)

    score = [column(score_ref[k : k + 1, :]) for k in range(top)]
    chosen = [
        column(chosen_ref[k : k + 1, :].astype(F32)).astype(jnp.int32) for k in range(top)
    ]
    whole = sum(score)
    lane = lax.broadcasted_iota(jnp.int32, (length, experts), 1)
    named = [chosen[k] == lane for k in range(top)]
    counted = sum(jnp.where(one, 1.0, 0.0) for one in named)
    before = (
        lax.broadcasted_iota(jnp.int32, (length, length), 0)
        > lax.broadcasted_iota(jnp.int32, (length, length), 1)
    )
    ranks = jnp.dot(
        jnp.where(before, 1.0, 0.0).astype(BF16), counted.astype(BF16),
        preferred_element_type=F32,
    )
    grid = lax.broadcasted_iota(jnp.int32, (length, experts * capacity), 1)
    pick = weight = 0.0
    for k, one in enumerate(named):
        rank = jnp.sum(jnp.where(one, ranks, 0.0), axis=1, keepdims=True).astype(jnp.int32)
        hit = grid == (chosen[k] ^ place_ref[0]) * capacity + rank
        pick = pick + jnp.where(hit, 1.0, 0.0)
        weight = weight + jnp.where(hit, score[k] / whole, 0.0)
    pick_ref[...] = jnp.transpose(pick).astype(BF16)
    high = weight.astype(BF16)
    high_ref[...] = high
    low_ref[...] = (weight - high.astype(F32)).astype(BF16)


def route(place, chosen, score, experts, capacity):
    length = chosen.shape[0]
    weight = jax.ShapeDtypeStruct((length, experts * capacity), BF16)
    args = (chosen.T, score.T)
    return pl.pallas_call(
        staged(lambda *refs: route_kernel(experts, capacity, *refs), 1, len(args)),
        in_specs=[pl.BlockSpec(memory_space=pltpu.SMEM)] + hbm(2),
        out_specs=vmem(3),
        scratch_shapes=stage(args),
        out_shape=[jax.ShapeDtypeStruct((experts * capacity, length), BF16), weight, weight],
        compiler_params=pltpu.CompilerParams(vmem_limit_bytes=8 * 2**20),
        name="route",
    )(place, *in_hbm(args))


def pack_kernel(*refs):
    height = refs[0].shape[0]
    for i, ref in enumerate(refs[:-1]):
        refs[-1][i * height : (i + 1) * height] = ref[...]


def pack(parts):
    height, wide = parts[0].shape
    return pl.pallas_call(
        pack_kernel,
        in_specs=vmem(len(parts)),
        out_specs=vmem(1)[0],
        out_shape=jax.ShapeDtypeStruct((height * len(parts), wide), BF16),
        compiler_params=pltpu.CompilerParams(vmem_limit_bytes=4 * 2**20),
        name="pack",
    )(*parts)


def project_kernel(count, *refs):
    skip_ref, pick_ref, stream_ref, *rows = refs[count:]
    total = refs[0][...]
    for ref in refs[1:count]:
        total = total + ref[...].astype(F32)
    stream = (skip_ref[...].astype(F32) + total.astype(BF16).astype(F32)).astype(BF16)
    stream_ref[...] = stream
    picked = jnp.dot(pick_ref[...], stream, preferred_element_type=F32).astype(BF16)
    height = rows[0].shape[0]
    for k, ref in enumerate(rows):
        ref[...] = picked[k * height : (k + 1) * height]


def project(sums, skip, pick, experts):
    length, d_local = skip.shape
    return pl.pallas_call(
        lambda *refs: project_kernel(len(sums), *refs),
        in_specs=vmem(len(sums) + 2),
        out_specs=vmem(1 + experts),
        out_shape=[jax.ShapeDtypeStruct((length, d_local), BF16)]
        + [jax.ShapeDtypeStruct((pick.shape[0] // experts, d_local), BF16)] * experts,
        compiler_params=pltpu.CompilerParams(vmem_limit_bytes=8 * 2**20),
        name="project",
    )(*sums, skip, pick)


def fold_kernel(pairs, *refs):
    outs = refs[2 * pairs :]
    share = len(outs) // pairs
    for i in range(pairs):
        total = (refs[i][...].astype(F32) + refs[pairs + i][...].astype(F32)).astype(BF16)
        height = outs[i * share].shape[0]
        for j in range(share):
            outs[i * share + j][...] = total[j * height : (j + 1) * height]


def fold(kept, moved, share):
    rows, wide = kept[0].shape
    return pl.pallas_call(
        lambda *refs: fold_kernel(len(kept), *refs),
        in_specs=vmem(2 * len(kept)),
        out_specs=vmem(len(kept) * share),
        out_shape=[jax.ShapeDtypeStruct((rows // share, wide), BF16)] * (len(kept) * share),
        compiler_params=pltpu.CompilerParams(vmem_limit_bytes=6 * 2**20),
        name="fold",
    )(*kept, *moved)


def combine_kernel(stream_ref, high_ref, low_ref, *refs):
    out_ref = refs[-1]
    total = stream_ref[...].astype(F32)
    back = jnp.concatenate([ref[...] for ref in refs[:-1]], axis=0)
    total = total + jnp.dot(high_ref[...], back, preferred_element_type=F32)
    total = total + jnp.dot(low_ref[...], back, preferred_element_type=F32)
    out_ref[...] = total.astype(BF16)


def combine(stream, high, low, back):
    return pl.pallas_call(
        combine_kernel,
        in_specs=vmem(3 + len(back)),
        out_specs=vmem(1)[0],
        out_shape=jax.ShapeDtypeStruct(stream.shape, BF16),
        compiler_params=pltpu.CompilerParams(vmem_limit_bytes=8 * 2**20),
        name="combine",
    )(stream, high, low, *back)


def ffn_kernel(n_tp, groups, width, place_ref, *refs):
    pieces = refs[: n_tp * groups]
    scale_ref, gate_ref, up_ref, down_ref = refs[n_tp * groups : n_tp * groups + 4]
    outs = refs[n_tp * groups + 4 :]
    me = place_ref[1]
    d_local = pieces[0].shape[1]
    square = gate = up = 0.0
    for k in range(n_tp):
        parts = [pieces[g * n_tp + k][...] for g in range(groups)]
        rows = jnp.concatenate(parts, axis=0).astype(F32)
        square = square + jnp.sum(rows * rows, axis=1, keepdims=True)
        place = pl.multiple_of((me ^ k) * d_local, d_local)
        scaled = (rows * scale_ref[me ^ k]).astype(BF16)
        gate = gate + jnp.dot(
            scaled, gate_ref[pl.ds(place, d_local), :], preferred_element_type=F32
        )
        up = up + jnp.dot(scaled, up_ref[pl.ds(place, d_local), :], preferred_element_type=F32)
    inv_rms = lax.rsqrt(square / width + EPS)
    gate = gate * inv_rms
    hidden = (gate * jax.nn.sigmoid(gate) * (up * inv_rms)).astype(BF16)
    for k in range(n_tp):
        place = pl.multiple_of((me ^ k) * d_local, d_local)
        done = jnp.dot(
            hidden, down_ref[:, pl.ds(place, d_local)], preferred_element_type=F32
        ).astype(BF16)
        start = 0
        for g in range(groups):
            out = outs[g * n_tp + k]
            out[...] = done[start : start + out.shape[0]]
            start += out.shape[0]


def load_kernel(*refs):
    half = len(refs) // 2
    sems = refs[-1]
    copies = [
        pltpu.make_async_copy(refs[i], refs[half + i], sems.at[i]) for i in range(half)
    ]
    for copy in copies:
        copy.start()
    for copy in copies:
        copy.wait()


def load(*weights):
    return pl.pallas_call(
        load_kernel,
        in_specs=hbm(len(weights)),
        out_specs=vmem(len(weights)),
        out_shape=[jax.ShapeDtypeStruct(w.shape, w.dtype) for w in weights],
        scratch_shapes=[pltpu.SemaphoreType.DMA((len(weights),))],
        compiler_params=pltpu.CompilerParams(vmem_limit_bytes=16 * 2**20),
        name="load",
    )(*in_hbm(weights))


def ffn(place, grouped, scale, gate_w, up_w, down_w):
    n_tp, groups = len(grouped[0]), len(grouped)
    pieces = [piece for group in grouped for piece in group]
    rows = sum(group[0].shape[0] for group in grouped)
    width, units = gate_w.shape
    outs = pl.pallas_call(
        lambda *refs: ffn_kernel(n_tp, groups, width, *refs),
        in_specs=[pl.BlockSpec(memory_space=pltpu.SMEM)] + vmem(len(pieces) + 4),
        out_specs=vmem(len(pieces)),
        out_shape=[jax.ShapeDtypeStruct(piece.shape, BF16) for piece in pieces],
        compiler_params=pltpu.CompilerParams(vmem_limit_bytes=24 * 2**20),
        cost_estimate=pl.CostEstimate(
            flops=6 * rows * width * units,
            bytes_accessed=6 * width * units + 4 * rows * width,
            transcendentals=rows * units,
        ),
        name="expert_ffn",
    )(place, *pieces, scale, gate_w, up_w, down_w)
    return [outs[g * n_tp : (g + 1) * n_tp] for g in range(groups)]


def gather_pieces(own, n_tp):
    pieces = {0: own}
    bit = n_tp // 2
    while bit:
        for k in list(pieces):
            pieces[k ^ bit] = swap(pieces[k], "tp", bit)
        bit //= 2
    return [pieces[k] for k in range(n_tp)]


def scatter_sum(parts, n_tp, share):
    held = {k: parts[k] for k in range(n_tp)}
    bit = 1
    while bit < n_tp:
        sent = sorted((k for k in held if k & bit), reverse=True)
        moved = []
        for k in sent:
            moved.append(swap(held[k], "tp", bit))
        last = 2 * bit == n_tp
        sums = fold([held[k ^ bit] for k in sent], moved, share if last else 1)
        if last:
            return sums
        held = {k ^ bit: total for k, total in zip(sent, sums)}
        bit *= 2
    return [parts[0]]


def layer(
    lane_source_signal,
    spectral_damping_part,
    spectral_angular_part,
    interval_exponent,
    entry_matrix_inphase,
    entry_matrix_quadrature,
    emission_inphase,
    emission_quadrature,
    lane_bypass_factor,
    spike_shrink_offset,
    lane_exit_matrix,
    skipline_stream,
    specialist_scaling_vector,
    selected_specialists,
    dispatcher_scores,
    specialist_valve_matrix,
    specialist_widen_matrix,
    specialist_shrink_matrix,
):
    n_tp, experts = lax.axis_size("tp"), lax.axis_size("sp")
    d_local = specialist_scaling_vector.shape[0] // n_tp
    tok_local, top = selected_specialists.shape
    capacity = 2 * tok_local * top // experts
    place = jnp.stack([lax.axis_index("sp"), lax.axis_index("tp")]).astype(jnp.int32)
    args = mixer_args(
        lane_source_signal,
        spectral_damping_part,
        spectral_angular_part,
        interval_exponent,
        entry_matrix_inphase,
        entry_matrix_quadrature,
        emission_inphase,
        emission_quadrature,
        lane_bypass_factor,
        spike_shrink_offset,
    )
    evens, odd, own_skip = cut_blocks(place, lane_exit_matrix, skipline_stream, n_tp)
    odd = swap(odd, "tp", 1)
    mixed = mixer(place, args)
    other = swap(mixed, "tp", 1)
    held = dict(zip(range(0, n_tp, 2), partial_sums(mixed, other, odd, evens)))
    sums = [held[0]]
    bit = 2
    while bit < n_tp:
        for k in [k for k in held if k & bit]:
            moved = swap(held.pop(k), "tp", bit)
            if k == bit:
                sums.append(moved)
            else:
                held[k ^ bit] = (held[k ^ bit].astype(F32) + moved.astype(F32)).astype(BF16)
        bit *= 2
    pick, high, low = route(place, selected_specialists, dispatcher_scores, experts, capacity)
    gate_w, up_w = load(specialist_valve_matrix[0], specialist_widen_matrix[0])
    (down_w,) = load(specialist_shrink_matrix[0])
    scale = specialist_scaling_vector.reshape(n_tp, 1, d_local)

    stream, *rows = project(sums, own_skip, pick, experts)
    arrived = {}
    for k in range(experts):
        arrived[k] = swap(rows[k], "sp", k) if k else rows[k]
    chunks = chunks_of(experts)
    pieces = []
    for chunk in chunks:
        own = [arrived[k] for k in chunk]
        pieces.append(gather_pieces(pack(own) if len(own) > 1 else own[0], n_tp))
    parts = []
    for members in calls_of(len(chunks)):
        parts += ffn(place, [pieces[i] for i in members], scale, gate_w, up_w, down_w)
    back = {}
    for c, chunk in enumerate(chunks):
        sums = scatter_sum(parts[c], n_tp, len(chunk))
        for k, total in zip(chunk, sums):
            back[k] = swap(total, "sp", k) if k else total
    return combine(stream, high, low, [back[k] for k in range(experts)])


def chunks_of(experts):
    half, part = experts // 2, experts // 4
    cuts = [0, max(1, experts // 8), half, half + part, experts]
    return [list(range(a, b)) for a, b in zip(cuts, cuts[1:])]


def calls_of(chunks):
    return [(0, 1)] + [(c,) for c in range(2, chunks)]


def solution(mesh):
    placed = (
        P("tp", "sp"),
        P("tp", None),
        P("tp", None),
        P("tp"),
        P("tp", None, None),
        P("tp", None, None),
        P("tp", None, None),
        P("tp", None, None),
        P("tp"),
        P("tp", "sp"),
        P("tp", None),
        P("sp", None),
        P(),
        P("sp", None),
        P("sp", None),
        P("sp", None, "tp"),
        P("sp", None, "tp"),
        P("sp", "tp", None),
    )
    return jax.shard_map(
        layer, mesh=mesh, in_specs=placed, out_specs=P("sp", "tp"), check_vma=False
    )
```
